32 devices in a mesh: kv: 8 (over z, x), tp: 4 (over y, core).
Axes of the slice: x: 2, y: 2, z: 4, core: 2. Of those that a mesh axis runs over, the one named last changes fastest.
Arguments:
- tokens: bfloat16 [256, 4096], P('kv', 'tp'), may hold values from -12 to 12
- norm_gain: float32 [4096], replicated, may hold values from 0.1 to 1.9
- query_weight: bfloat16 [4096, 4096], P('kv', 'tp'), may hold values from -0.09375 to 0.09375
- key_weight: bfloat16 [4096, 4096], P('kv', 'tp'), may hold values from -0.09375 to 0.09375
- value_weight: bfloat16 [4096, 4096], P('kv', 'tp'), may hold values from -0.09375 to 0.09375
- outgate_weight: bfloat16 [4096, 4096], P('kv', 'tp'), may hold values from -0.09375 to 0.09375
- ingate_weight: bfloat16 [4096, 16], replicated, may hold values from -0.09375 to 0.09375
- forget_weight: bfloat16 [4096, 16], replicated, may hold values from -0.09375 to 0.09375
- forget_bias: float32 [16], replicated, may hold values from 0.5 to 4
- output_weight: bfloat16 [4096, 4096], P('tp', 'kv'), may hold values from -0.09375 to 0.09375
- state_memory: float32 [64, 16, 256, 256], P('kv', 'tp'), may hold values from -0.8 to 0.8
- state_normaliser: float32 [64, 16, 256], P('kv', 'tp'), may hold values from -0.8 to 0.8
- state_stabiliser: float32 [64, 16], P('kv', 'tp'), may hold values from -4 to 4
- past_keys: bfloat16 [64, 4, 4096], P('kv', None, 'tp'), may hold values from -6 to 6
- past_values: bfloat16 [64, 4, 4096], P('kv', None, 'tp'), may hold values from -6 to 6
- past_ingate: float32 [64, 4, 16], P('kv', None, 'tp'), may hold values from -4 to 4
- past_forget: float32 [64, 4, 16], P('kv', None, 'tp'), may hold values from -1 to 4
- accepted: int32 [64], P('kv'), may hold values from 0 to 4
Outputs:
- mixed: bfloat16 [256, 4096], P('kv', 'tp')
- taken_memory: float32 [64, 16, 256, 256], P('kv', 'tp')
- taken_normaliser: float32 [64, 16, 256], P('kv', 'tp')
- taken_stabiliser: float32 [64, 16], P('kv', 'tp')
- new_keys: bfloat16 [256, 4096], P('kv', 'tp')
- new_values: bfloat16 [256, 4096], P('kv', 'tp')
The draws below stay inside these ranges and needn't reach their ends.
All inputs are finite; a program needn't handle non-finite values.
Results may differ from the reference program's by a relative error of at most 0.03.
Values may be sent and summed in bfloat16 or wider, within the bound.
A program may use at most 64 MiB of HBM per device.

```python
import jax
import jax.numpy as jnp
from jax import lax

D = 4096
HEADS = 16
DK = 256
DV = 256
PROPS = 4
SEQS = 64
TOKENS = 256
HD = 4096
N_TP = 4


def draw_tokens(key, part):
    base_key = jax.random.fold_in(key, 11)
    scale_key = jax.random.fold_in(key, 12)
    base_values = jnp.clip(jax.random.normal(base_key, (TOKENS, D), jnp.float32), -4.0, 4.0)
    levels = jax.random.uniform(scale_key, (TOKENS, 32), jnp.float32, jnp.log(0.3), jnp.log(3.0))
    block_scale = jnp.repeat(jnp.exp(levels), D // 32, axis=1)
    return (base_values * block_scale).astype(jnp.bfloat16)


def touch_ends(array, stream_key, smallest, top_value):
    index_at = [jax.random.randint(jax.random.fold_in(stream_key, axis), (), 0, length) for axis, length in enumerate(array.shape)]
    widest = array.shape.index(max(array.shape))
    beside = index_at[:widest] + [(index_at[widest] + 1) % array.shape[widest]] + index_at[widest + 1:]
    return array.at[tuple(index_at)].set(smallest).at[tuple(beside)].set(top_value)


def level_of(rng, shape, shards, least, high):
    def one(position, parts):
        steps = jax.random.uniform(jax.random.fold_in(jax.random.fold_in(rng, 6), position), (parts,), jnp.float32, least / len(shards), high / len(shards))
        return jnp.repeat(jnp.exp(steps), shape[position] // parts).reshape((-1,) + (1,) * (len(shape) - position - 1))

    gain = one(*shards[0])
    for cut in shards[1:]:
        gain = gain * one(*cut)
    return gain


def scatter_about(rng, dims, spread, most, pieces=(), held_as=jnp.bfloat16):
    array = jax.random.normal(rng, dims, jnp.float32) * spread
    if len(pieces) > 0:
        array = level_of(rng, dims, pieces, -0.22, 0.18) * array
    return jnp.clip(array, min=-most, max=most).astype(held_as)


def setup_inputs(seed: int = 0) -> dict:
    keys = jax.random.split(jax.random.key(seed), 19)
    tokens = draw_tokens(jax.random.fold_in(keys[18], 71), 0)
    norm_gain = jnp.clip(1.0 + 0.18 * jax.random.normal(keys[1], (D,), jnp.float32), 0.1, 1.9)
    query_weight = scatter_about(keys[2], (D, HD), D ** -0.5, 0.09375, ((0, 8), (1, 4)))
    key_weight = scatter_about(keys[3], (D, HD), D ** -0.5, 0.09375, ((0, 8), (1, 4)))
    value_weight = scatter_about(keys[4], (D, HD), D ** -0.5, 0.09375, ((0, 8), (1, 4)))
    outgate_weight = scatter_about(keys[5], (D, HD), D ** -0.5, 0.09375, ((0, 8), (1, 4)))
    ingate_weight = scatter_about(keys[6], (D, HEADS), D ** -0.5, 0.09375)
    forget_weight = scatter_about(keys[7], (D, HEADS), D ** -0.5, 0.09375)
    forget_bias = jnp.clip(jax.random.uniform(keys[8], (HEADS,), jnp.float32, 0.5, 4.0), 0.5, 4.0)
    output_weight = scatter_about(keys[9], (HD, D), HD ** -0.5, 0.09375, ((0, 4), (1, 8)))
    state_memory = scatter_about(keys[10], (SEQS, HEADS, DK, DV), 0.1, 0.8, ((0, 8), (1, 4)), jnp.float32)
    state_normaliser = scatter_about(keys[11], (SEQS, HEADS, DK), 0.1, 0.8, ((0, 8), (1, 4)), jnp.float32)
    state_stabiliser = scatter_about(keys[12], (SEQS, HEADS), 1.0, 4.0, ((0, 8), (1, 4)), jnp.float32)
    past_keys = scatter_about(keys[13], (SEQS, PROPS, HD), 1.0, 6.0, ((0, 8), (2, 4)))
    past_values = scatter_about(keys[14], (SEQS, PROPS, HD), 1.0, 6.0, ((0, 8), (2, 4)))
    past_ingate = scatter_about(keys[15], (SEQS, PROPS, HEADS), 1.0, 4.0, ((0, 8), (2, 4)), jnp.float32)
    past_forget = jnp.clip(-1.0 + 5.0 * jax.random.uniform(keys[16], (SEQS, PROPS, HEADS), jnp.float32) ** level_of(keys[16], (SEQS, PROPS, HEADS), ((0, 8), (2, 4)), -0.2, 0.2), -1.0, 4.0)
    accepted = touch_ends(jax.random.randint(keys[17], (SEQS,), 0, PROPS + 1), jax.random.fold_in(keys[17], 1), 0, PROPS).astype(jnp.int32)
    return dict(tokens=tokens, norm_gain=norm_gain, query_weight=query_weight, key_weight=key_weight, value_weight=value_weight, outgate_weight=outgate_weight, ingate_weight=ingate_weight, forget_weight=forget_weight, forget_bias=forget_bias, output_weight=output_weight, state_memory=state_memory, state_normaliser=state_normaliser, state_stabiliser=state_stabiliser, past_keys=past_keys, past_values=past_values, past_ingate=past_ingate, past_forget=past_forget, accepted=accepted)


exact_mode = lax.Precision.HIGHEST
epsilon = 1e-06

def rounded(values):
    return lax.optimization_barrier(values.astype(jnp.bfloat16))

def heads_view(rows, seq_count, head_count):
    shaped = rows.astype(jnp.float32).reshape(seq_count, -1, head_count, rows.shape[-1] // head_count)
    return shaped.transpose(0, 2, 1, 3)

def catch_up(memory, normaliser, stabiliser, key_rows, values, in_gate, forget_pre, taken_mask):
    log_forget = jnp.where(taken_mask, jax.nn.log_sigmoid(forget_pre), 0.0)
    running = jnp.cumsum(log_forget, axis=-1)
    chain_total = running[..., -1]
    end_logs = jnp.where(taken_mask, chain_total[..., None] - running + in_gate, -jnp.inf)
    stable_new = jnp.maximum(chain_total + stabiliser, lax.optimization_barrier(jnp.max(end_logs, axis=-1)))
    carry_decay = jnp.exp(chain_total + stabiliser - stable_new)
    weighted = key_rows * jnp.exp(end_logs - stable_new[..., None])[..., None]
    memory_new = carry_decay[..., None, None] * memory + jnp.einsum('...pd,...pe->...de', weighted, values, precision=exact_mode)
    normaliser_new = carry_decay[..., None] * normaliser + lax.optimization_barrier(jnp.sum(weighted, axis=-2))
    return (memory_new, normaliser_new, stable_new)

def advance(memory, normaliser, stabiliser, query_rows, key_rows, values, in_gate, forget_pre):
    chain_len = query_rows.shape[-2]
    running = jnp.cumsum(jax.nn.log_sigmoid(forget_pre), axis=-1)
    causal = jnp.arange(chain_len)[:, None] >= jnp.arange(chain_len)[None, :]
    within = jnp.where(causal, running[..., :, None] - running[..., None, :] + in_gate[..., None, :], -jnp.inf)
    carried = running + stabiliser[..., None]
    stable = jnp.maximum(carried, lax.optimization_barrier(jnp.max(within, axis=-1)))
    scores = jnp.einsum('...td,...sd->...ts', query_rows, key_rows, precision=exact_mode) * jnp.exp(within - stable[..., None])
    carry_weight = jnp.exp(carried - stable)
    numerator = carry_weight[..., None] * jnp.einsum('...td,...de->...te', query_rows, memory, precision=exact_mode)
    numerator = numerator + jnp.einsum('...ts,...se->...te', scores, values, precision=exact_mode)
    denominator = carry_weight * jnp.einsum('...td,...d->...t', query_rows, normaliser, precision=exact_mode) + lax.optimization_barrier(jnp.sum(scores, axis=-1))
    return numerator / jnp.maximum(jnp.abs(denominator), 1.0)[..., None]

def reference(tokens, norm_gain, query_weight, key_weight, value_weight, outgate_weight, ingate_weight, forget_weight, forget_bias, output_weight, state_memory, state_normaliser, state_stabiliser, past_keys, past_values, past_ingate, past_forget, accepted):
    floats = tokens.astype(jnp.float32)
    squares = lax.optimization_barrier(jnp.sum(floats * floats, axis=1, keepdims=True))
    normed = (floats * lax.rsqrt(squares / D + epsilon) * norm_gain).astype(jnp.bfloat16)
    query_b = rounded(jnp.dot(normed, query_weight, preferred_element_type=jnp.float32))
    key_b = rounded(jnp.dot(normed, key_weight, preferred_element_type=jnp.float32))
    value_b = rounded(jnp.dot(normed, value_weight, preferred_element_type=jnp.float32))
    outgate_b = rounded(jnp.dot(normed, outgate_weight, preferred_element_type=jnp.float32))
    in_gate = jnp.dot(normed, ingate_weight, preferred_element_type=jnp.float32)
    forget_pre = jnp.dot(normed, forget_weight, preferred_element_type=jnp.float32) + forget_bias
    seq_count = past_keys.shape[0]
    chain_len = past_keys.shape[1]
    key_scale = DK ** (-0.5)
    query_h = heads_view(query_b, seq_count, HEADS)
    key_h = heads_view(key_b, seq_count, HEADS) * key_scale
    value_h = heads_view(value_b, seq_count, HEADS)
    outgate_h = heads_view(outgate_b, seq_count, HEADS)
    in_h = in_gate.reshape(seq_count, chain_len, HEADS).transpose(0, 2, 1)
    forget_h = forget_pre.reshape(seq_count, chain_len, HEADS).transpose(0, 2, 1)
    past_key_h = heads_view(past_keys, seq_count, HEADS) * key_scale
    past_value_h = heads_view(past_values, seq_count, HEADS)
    past_in_h = past_ingate.transpose(0, 2, 1)
    past_forget_h = past_forget.transpose(0, 2, 1)

    def per_sequence(items):
        memory, normaliser, stabiliser, query_s, key_s, value_s, outgate_s, in_s, forget_s, past_key_s, past_value_s, past_in_s, past_forget_s, taken_count = items
        taken_mask = (jnp.arange(chain_len) < taken_count)[None, :]
        memory_new, normaliser_new, stable_new = catch_up(memory, normaliser, stabiliser, past_key_s, past_value_s, past_in_s, past_forget_s, taken_mask)
        hidden = advance(memory_new, normaliser_new, stable_new, query_s, key_s, value_s, in_s, forget_s)
        gated = (jax.nn.sigmoid(outgate_s) * hidden).transpose(1, 0, 2).reshape(chain_len, -1).astype(jnp.bfloat16)
        return (memory_new, normaliser_new, stable_new, gated)
    memory_out, normaliser_out, stable_out, gated_all = lax.map(per_sequence, (state_memory, state_normaliser, state_stabiliser, query_h, key_h, value_h, outgate_h, in_h, forget_h, past_key_h, past_value_h, past_in_h, past_forget_h, accepted))
    gated_rows = gated_all.reshape(seq_count * chain_len, -1)
    groups = gated_rows.reshape(gated_rows.shape[0], N_TP, -1).transpose(1, 0, 2)
    weight_groups = output_weight.reshape(N_TP, -1, D)

    def add_group(running_sum, group_pair):
        group_sum = lax.optimization_barrier(jnp.dot(group_pair[0], group_pair[1], preferred_element_type=jnp.float32).astype(jnp.bfloat16))
        return (running_sum + group_sum.astype(jnp.float32), None)
    running_sum, ignored = lax.scan(add_group, jnp.zeros((gated_rows.shape[0], D), jnp.float32), (groups, weight_groups))
    mixed = running_sum.astype(jnp.bfloat16)
    return (mixed, memory_out, normaliser_out, stable_out, key_b, value_b)
```

```python
import functools

import jax
import jax.numpy as jnp
from jax import lax
from jax.experimental import pallas as pl
from jax.experimental.pallas import tpu as pltpu
from jax.sharding import PartitionSpec as P

epsilon = 1e-06
MESH = pl.DeviceIdType.MESH
vmem = pl.BlockSpec(memory_space=pltpu.VMEM)
hbm = pl.BlockSpec(memory_space=pltpu.HBM)
f32 = jnp.float32
bf16 = jnp.bfloat16
DMA = pltpu.SemaphoreType.DMA


def signal(sem, kv, tp):
    pl.semaphore_signal(sem, inc=1, device_id={"kv": kv, "tp": tp}, device_id_type=MESH)


def remote(src, dst, send_sem, recv_sem, kv, tp):
    return pltpu.make_async_remote_copy(
        src_ref=src,
        dst_ref=dst,
        send_sem=send_sem,
        recv_sem=recv_sem,
        device_id={"kv": kv, "tp": tp},
        device_id_type=MESH,
    )


def each(count, step, start=0):
    def run(index, carry):
        step(index)
        return carry

    lax.fori_loop(start, count, run, 0)


def log_sigmoid(v):
    return jnp.minimum(v, 0.0) - jnp.log1p(jnp.exp(-jnp.abs(v)))


def iota(shape, axis):
    return lax.broadcasted_iota(jnp.int32, shape, axis)


def cell_kernel(
    n, m, all_heads, features, chain,
    tok_h, gain_h, wi_h, wf_h, bias_h, w0_h, w1_h, w2_h, w3_h, wo_h,
    memory_h, norm_h, stab_h, past_k_h, past_v_h, past_i_h, past_f_h, taken_h,
    mixed, key_b, value_b, memory, norm_new, stab_new,
    tok, gain, wg, bias, w_in, w_out, norm, stab, past_k, past_v, past_i, past_f, taken,
    x_buf, xs, keep, give, near, pair, far, g_own, g_buf,
    m_low, weights, decay, query_b, outgate_b, from_memory, gated,
    a_buf, p_buf, q_buf, o_send, o_buf,
    in_sem, w_sem, m_sem, t_send, f_send, x_recv, g_send, g_recv,
    n_send, n_recv, z_send, z_recv, a_send, a_recv, p_send, p_recv, o_ssem, o_rsem,
):
    k = lax.axis_index("kv")
    t = lax.axis_index("tp")
    r = n // m
    half = n // 2
    pairs = m // 2
    rows, local = tok.shape
    width = xs.shape[2]
    cols = w_in.shape[2]
    out_cols = w_out.shape[1]
    seqs, heads, dk, dv = memory.shape
    z = k // 2
    x = k % 2
    core = t % 2
    partner = t + 1 - 2 * core
    beside = z * 2 + 1 - x
    t0 = k // r
    mine = k % r
    root = t0 == t
    root_core = t0 % 2 == core
    turn = 1 - 2 * (z // max(half // 2, 1))

    def plane(i):
        return lax.rem(z + i * turn + half, half)

    small = [
        pltpu.make_async_copy(tok_h, tok, in_sem.at[0]),
        pltpu.make_async_copy(gain_h, gain, in_sem.at[1]),
        pltpu.make_async_copy(
            wi_h.at[:, pl.ds(pl.multiple_of(t * local, local), local)],
            wg.at[pl.ds(0, all_heads)], in_sem.at[2],
        ),
        pltpu.make_async_copy(
            wf_h.at[:, pl.ds(pl.multiple_of(t * local, local), local)],
            wg.at[pl.ds(all_heads, all_heads)], in_sem.at[3],
        ),
    ]
    late = [
        pltpu.make_async_copy(src, dst, in_sem.at[4 + i])
        for i, (src, dst) in enumerate((
            (bias_h, bias), (norm_h, norm), (stab_h, stab), (past_k_h, past_k),
            (past_v_h, past_v), (past_i_h, past_i), (past_f_h, past_f), (taken_h, taken),
        ))
    ]
    big = [
        pltpu.make_async_copy(src, w_in.at[i], w_sem.at[i])
        for i, src in enumerate((w0_h, w1_h, w2_h, w3_h))
    ]
    load_out = pltpu.make_async_copy(wo_h, w_out, w_sem.at[4])

    def load(q):
        return pltpu.make_async_copy(memory_h.at[q], memory.at[q], m_sem.at[q])

    for copy in small + big + late:
        copy.start()
    load_out.start()
    each(seqs, lambda q: load(q).start())

    barrier = pltpu.get_barrier_semaphore()
    each(n, lambda i: signal(barrier, lax.rem(k + i, n), t), 1)
    each(m, lambda j: signal(barrier, k, lax.rem(t + j, m)), 1)
    last_at = k % m

    def greet_last(h):
        kk = t * r + h

        @pl.when(jnp.logical_not(jnp.logical_and(kk == k, last_at == t)))
        def _():
            signal(barrier, kk, last_at)

    each(r, greet_last)
    both = jnp.logical_and(root, last_at == t).astype(jnp.int32)
    pl.semaphore_wait(barrier, (n - 1) + (m - 1) + r - both)

    small[0].wait()

    def token_copy(h):
        cut = pl.ds(pl.multiple_of(h * width, width), width)
        return remote(tok.at[:, cut], x_buf.at[k], t_send.at[h], x_recv.at[k], t * r + h, t)

    def own_token(h):
        return jnp.logical_and(root, h == mine)

    def start_token(h):
        @pl.when(jnp.logical_not(own_token(h)))
        def _():
            token_copy(h).start()

    each(r, start_token)

    @pl.when(root)
    def _():
        x_buf[k] = tok[:, pl.ds(pl.multiple_of(mine * width, width), width)]

    def forward(j, i, to):
        return remote(x_buf.at[j], x_buf.at[j], f_send.at[i, j], x_recv.at[j], k, to)

    def cousin(i):
        return lax.rem(t + 2 * i, m)

    def pass_token(j):
        @pl.when(jnp.logical_not(jnp.logical_and(root, j == k)))
        def _():
            remote(
                tok.at[:, pl.ds(0, width)], x_buf.at[j], t_send.at[0], x_recv.at[j], k, t
            ).wait_recv()

        @pl.when(root)
        def _():
            for i in range(1, pairs):
                forward(j, i, cousin(i)).start()

        @pl.when(root_core)
        def _():
            forward(j, 0, partner).start()

    wg[pl.ds(2 * all_heads, wg.shape[0] - 2 * all_heads), :] = jnp.zeros(
        (wg.shape[0] - 2 * all_heads, local), bf16
    )
    for copy in small[1:]:
        copy.wait()
    floats = tok[...].astype(f32)
    squares = jnp.sum(floats * floats, axis=1, keepdims=True)
    lifted = floats * gain[:, pl.ds(pl.multiple_of(t * local, local), local)]
    raw = lax.dot_general(
        lifted.astype(bf16), wg[...], (((1,), (1,)), ((), ())), preferred_element_type=f32
    )
    lane = iota(raw.shape, 1)
    g_own[...] = jnp.where(lane < 2 * all_heads, raw, squares)

    def gate_copy(j):
        return remote(
            g_own, g_buf.at[j - 1], g_send.at[j - 1], g_recv.at[j - 1], k, lax.rem(t + j, m)
        )

    each(m, lambda j: gate_copy(j).start(), 1)
    own_gain = gain[:, pl.ds(pl.multiple_of(k * width, width), width)]

    def scale_plane(p):
        for side, j in enumerate((p * 2 + x, p * 2 + 1 - x)):
            xs[p, side * rows : (side + 1) * rows, :] = (
                x_buf[j].astype(f32) * own_gain
            ).astype(bf16)

    def near_copy(c, p):
        return remote(
            give.at[c, p], near.at[c, p], n_send.at[c, p], n_recv.at[c, p], beside, t
        )

    def project(c, p):
        part = jnp.dot(xs[p], w_in[c], preferred_element_type=f32)
        give[c, p] = part[rows:].astype(bf16)
        near_copy(c, p).start()
        keep[c, p] = part[:rows].astype(bf16)

    def take_plane(p):
        pass_token(p * 2 + x)
        pass_token(p * 2 + 1 - x)
        scale_plane(p)

    take_plane(z)
    for c in range(2):
        big[c].wait()
        project(c, z)
    for c in range(2, 4):
        big[c].wait()

    def far_plane(i):
        p = plane(i)
        take_plane(p)
        for c in range(4):
            project(c, p)

    each(half, far_plane, 1)
    for c in range(2, 4):
        project(c, z)

    for copy in late:
        copy.wait()
    key_scale = dk ** (-0.5)
    reach = taken[...]
    chain_sum = jnp.zeros((heads, seqs), f32)
    running = []
    for j in range(chain):
        chain_sum = chain_sum + jnp.where(j < reach, log_sigmoid(past_f[j]), 0.0)
        running.append(chain_sum)
    carried_log = chain_sum + stab[...]
    new_stab = carried_log
    ends = []
    for j in range(chain):
        ends.append(jnp.where(j < reach, chain_sum - running[j] + past_i[j], -jnp.inf))
        new_stab = jnp.maximum(new_stab, ends[j])
    stab_new[...] = new_stab
    decay[...] = jnp.exp(carried_log - new_stab)
    for j in range(chain):
        weight_j = jnp.exp(ends[j] - new_stab)
        for h in range(heads):
            weights[h, j : j + 1, :] = weight_j[h : h + 1, :]

    def take(q):
        load(q).wait()
        for h in range(heads):
            at = slice(h * dk, (h + 1) * dk)
            w_col = jnp.sum(
                jnp.where(iota((chain, seqs), 1) == q, weights[h], 0.0), axis=1, keepdims=True
            )
            fade = jnp.sum(
                jnp.where(iota((1, seqs), 1) == q, decay[h : h + 1, :], 0.0),
                axis=1, keepdims=True,
            )
            lifted_k = past_k[q, :, at].astype(f32) * key_scale * w_col
            norm_new[q, h : h + 1, :] = fade * norm[q, h : h + 1, :] + jnp.sum(
                lifted_k, axis=0, keepdims=True
            )
            added = lax.dot_general(
                lifted_k.astype(bf16),
                past_v[q, :, h * dv : (h + 1) * dv],
                (((0,), (0,)), ((), ())),
                preferred_element_type=f32,
            )
            new = fade * memory[q, h] + added
            memory[q, h] = new
            m_low[q, h] = new.astype(bf16)

    def fold(c, p):
        near_copy(c, p).wait_recv()
        pair[c, p] = (keep[c, p].astype(f32) + near[c, p].astype(f32)).astype(bf16)

    def far_copy(c, p):
        slot = lax.rem(z - p + half, half) - 1
        return remote(
            pair.at[c, p], far.at[c, slot], z_send.at[c, p], z_recv.at[c, slot], p * 2 + x, t
        )

    def fold_plane(i):
        p = plane(i)
        each(seqs * i // (half - 1), take, seqs * (i - 1) // (half - 1))
        for c in range(4):
            fold(c, p)
            far_copy(c, p).start()

    for c in range(2):
        fold(c, z)
    each(half, fold_plane, 1)

    def landed_far(c, i):
        remote(
            pair.at[c, 0], far.at[c, i], z_send.at[c, 0], z_recv.at[c, i], k, t
        ).wait_recv()

    each(m, lambda j: gate_copy(j).wait_recv(), 1)
    total = g_own[...]
    for j in range(m - 1):
        total = total + g_buf[j]
    scale = lax.rsqrt(total[:, 2 * all_heads : 2 * all_heads + 1] / features + epsilon)
    gates = total * scale

    def settle(c, out):
        each(half - 1, lambda i: landed_far(c, i))
        summed = pair[c, z].astype(f32)
        for i in range(half - 1):
            summed = summed + far[c, i].astype(f32)
        out[...] = (summed * scale).astype(bf16)

    settle(0, query_b)
    row_seq = iota((rows, dv), 0) // chain
    from_memory[...] = jnp.zeros(from_memory.shape, f32)

    def recall(q):
        for h in range(heads):
            at = slice(h * dv, (h + 1) * dv)
            got = jnp.dot(
                query_b[:, h * dk : (h + 1) * dk], m_low[q, h], preferred_element_type=f32
            )
            from_memory[:, at] = jnp.where(row_seq == q, got, from_memory[:, at])

    each(seqs, recall)
    settle(1, key_b)

    token_row = iota((rows, rows), 0)
    token_col = iota((rows, rows), 1)
    same_seq = token_row // chain == token_col // chain
    causal = jnp.logical_and(same_seq, token_col <= token_row)
    diagonal = token_row == token_col
    own_seq = iota((rows, seqs), 0) // chain == iota((rows, seqs), 1)
    first = t * heads

    def to_row(col):
        return jnp.sum(jnp.where(diagonal, col, 0.0), axis=0, keepdims=True)

    def pick(array, at):
        return jnp.sum(
            jnp.where(iota(array.shape, 1) == at, array, 0.0), axis=1, keepdims=True
        )

    scores, carries, dens = [], [], []
    for h in range(heads):
        at = slice(h * dk, (h + 1) * dk)
        in_col = pick(gates, first + h)
        forget = pick(gates, all_heads + first + h) + pick(bias[...], first + h)
        b_col = jnp.sum(
            jnp.where(causal, to_row(log_sigmoid(forget)), 0.0), axis=1, keepdims=True
        )
        within = jnp.where(causal, b_col + to_row(in_col - b_col), -jnp.inf)
        stab_col = jnp.sum(
            jnp.where(own_seq, stab_new[h : h + 1, :], 0.0), axis=1, keepdims=True
        )
        carried = b_col + stab_col
        stable = jnp.maximum(carried, jnp.max(within, axis=1, keepdims=True))
        carry = jnp.exp(carried - stable)
        match = lax.dot_general(
            query_b[:, at], key_b[:, at], (((1,), (1,)), ((), ())), preferred_element_type=f32
        )
        score = match * key_scale * jnp.exp(within - stable)
        across_n = lax.dot_general(
            query_b[:, at].astype(f32), norm_new[:, h, :], (((1,), (1,)), ((), ())),
            precision=lax.Precision.HIGHEST, preferred_element_type=f32,
        )
        q_n = jnp.sum(jnp.where(own_seq, across_n, 0.0), axis=1, keepdims=True)
        den = carry * q_n + jnp.sum(score, axis=1, keepdims=True)
        scores.append(score.astype(bf16))
        carries.append(carry)
        dens.append(1.0 / jnp.maximum(jnp.abs(den), 1.0))

    for c in range(2, 4):
        fold(c, z)
    settle(2, value_b)
    for h in range(heads):
        at = slice(h * dv, (h + 1) * dv)
        fresh = jnp.dot(scores[h], value_b[:, at], preferred_element_type=f32)
        from_memory[:, at] = (carries[h] * from_memory[:, at] + fresh) * dens[h]
    settle(3, outgate_b)
    gated[...] = (jax.nn.sigmoid(outgate_b[...].astype(f32)) * from_memory[...]).astype(bf16)

    def along_copy(i):
        return remote(gated, a_buf.at[k], a_send.at[i], a_recv.at[k], plane(i) * 2 + x, t)

    def across_copy(i):
        at = plane(i) * 2 + x
        return remote(
            a_buf.at[at], a_buf.at[at], a_send.at[half + i], a_recv.at[at], beside, t
        )

    own_copy = remote(gated, a_buf.at[k], a_send.at[0], a_recv.at[k], beside, t)
    each(half, lambda i: along_copy(i).start(), 1)
    own_copy.start()
    a_buf[k] = gated[...]
    load_out.wait()

    def landed(at):
        remote(gated, a_buf.at[at], a_send.at[0], a_recv.at[at], k, t).wait_recv()

    def part_copy(kb):
        j = kb // m
        return remote(p_buf.at[kb], q_buf.at[j, t], p_send.at[kb], p_recv.at[j, t], k, kb % m)

    def away(kb):
        return kb % m != t

    def mix_plane(p):
        landed(p * 2 + 1 - x)
        both_rows = a_buf[pl.ds(p * 2, 2)].reshape(2 * rows, cols)
        part = jnp.dot(both_rows, w_out[...], preferred_element_type=f32).astype(bf16)
        for side in range(2):
            kb = p * 2 + side
            p_buf[kb] = part[side * rows : (side + 1) * rows]

            @pl.when(away(kb))
            def _():
                part_copy(kb).start()

    def step_plane(i):
        landed(plane(i) * 2 + x)
        across_copy(i).start()
        mix_plane(plane(i - 1))

    each(half, step_plane, 1)
    mix_plane(plane(half - 1))

    def final_copy(j):
        return remote(o_send.at[j], o_buf.at[mine], o_ssem.at[j], o_rsem.at[mine], j * m + t, t0)

    def stays(j):
        return jnp.logical_and(root, j * m + t == k)

    for j in range(r):
        def landed_part(tt, j=j):
            @pl.when(tt != t)
            def _():
                remote(
                    p_buf.at[0], q_buf.at[j, tt], p_send.at[0], p_recv.at[j, tt], k, t
                ).wait_recv()

        each(m, landed_part)
        q_buf[j, t] = p_buf[j * m + t]
        summed = q_buf[j, 0].astype(f32)
        for tt in range(1, m):
            summed = summed + q_buf[j, tt].astype(f32)
        o_send[j] = summed.astype(bf16)

        @pl.when(jnp.logical_not(stays(j)))
        def _(j=j):
            final_copy(j).start()

        @pl.when(stays(j))
        def _(j=j):
            o_buf[mine] = o_send[j]

    for h in range(r):
        @pl.when(jnp.logical_not(jnp.logical_and(t * r + h == k, last_at == t)))
        def _(h=h):
            remote(
                o_send.at[0], o_buf.at[h], o_ssem.at[0], o_rsem.at[h], k, t
            ).wait_recv()

        mixed[:, h * out_cols : (h + 1) * out_cols] = o_buf[h]

    def drain_token(h):
        @pl.when(jnp.logical_not(own_token(h)))
        def _():
            token_copy(h).wait_send()

    each(r, drain_token)

    def drain_forward(j):
        @pl.when(root)
        def _():
            for i in range(1, pairs):
                forward(j, i, cousin(i)).wait_send()

        @pl.when(root_core)
        def _():
            forward(j, 0, partner).wait_send()

    each(n, drain_forward)
    each(m, lambda j: gate_copy(j).wait_send(), 1)
    for c in range(4):
        each(half, lambda p, c=c: near_copy(c, p).wait_send())
        each(half, lambda i, c=c: far_copy(c, plane(i)).wait_send(), 1)
    each(half, lambda i: along_copy(i).wait_send(), 1)
    own_copy.wait_send()
    each(half, lambda i: across_copy(i).wait_send(), 1)

    def drain_part(kb):
        @pl.when(away(kb))
        def _():
            part_copy(kb).wait_send()

    each(n, drain_part)
    for j in range(r):
        @pl.when(jnp.logical_not(stays(j)))
        def _(j=j):
            final_copy(j).wait_send()


def cell(n, m, tokens, gain, wi, wf, bias, weights, w_out, memory, norm, stab, past_k, past_v,
         past_i, past_f, taken):
    seqs, heads, dk, dv = memory.shape
    rows, local = tokens.shape
    width, cols = weights[0].shape
    all_heads = wi.shape[0]
    chain = past_k.shape[1]
    depth, out_cols = w_out.shape
    half, r = n // 2, n // m
    lanes = -(-(2 * all_heads + 1) // 128) * 128
    row_block = jax.ShapeDtypeStruct((rows, cols), bf16)
    V = pltpu.VMEM
    outs = [
        V((rows, local), bf16), V((rows, cols), bf16), V((rows, cols), bf16),
        V(memory.shape, f32), V(norm.shape, f32), V(stab.shape, f32),
    ]
    return pl.pallas_call(
        functools.partial(cell_kernel, n, m, all_heads, local * m, chain),
        out_shape=outs,
        in_specs=[hbm] * 18,
        out_specs=[vmem] * 6,
        scratch_shapes=[
            V((rows, local), bf16), V(gain.shape, f32), V((lanes, local), bf16),
            V(bias.shape, f32), V((4, width, cols), bf16), V(w_out.shape, bf16),
            V(norm.shape, f32), V(stab.shape, f32), V(past_k.shape, bf16),
            V(past_v.shape, bf16), V(past_i.shape, f32), V(past_f.shape, f32),
            V(taken.shape, jnp.int32),
            V((n, rows, width), bf16), V((half, 2 * rows, width), bf16),
            V((4, half, rows, cols), bf16), V((4, half, rows, cols), bf16),
            V((4, half, rows, cols), bf16), V((4, half, rows, cols), bf16),
            V((4, half - 1, rows, cols), bf16),
            V((rows, lanes), f32), V((m - 1, rows, lanes), f32),
            V(memory.shape, bf16), V((heads, chain, seqs), f32), V(stab.shape, f32),
            V((rows, cols), bf16), V((rows, cols), bf16), V((rows, cols), f32),
            V((rows, cols), bf16),
            V((n, rows, cols), bf16), V((n, rows, out_cols), bf16),
            V((r, m, rows, out_cols), bf16), V((r, rows, out_cols), bf16),
            V((r, rows, out_cols), bf16),
            DMA((12,)), DMA((5,)), DMA((seqs,)), DMA((r,)), DMA((m // 2, n)), DMA((n,)),
            DMA((m - 1,)), DMA((m - 1,)),
            DMA((4, half)), DMA((4, half)), DMA((4, half)), DMA((4, half - 1)),
            DMA((n,)), DMA((n,)), DMA((n,)), DMA((r, m)), DMA((r,)), DMA((r,)),
        ],
        compiler_params=pltpu.CompilerParams(
            collective_id=0, has_side_effects=True, vmem_limit_bytes=40 * 1024 * 1024
        ),
    )(*(pltpu.with_memory_space_constraint(a, pltpu.HBM) for a in (
        tokens, gain, wi, wf, bias, *weights, w_out, memory, norm, stab, past_k, past_v,
        past_i, past_f, taken,
    )))


def put_kernel(count, pieces, *refs):
    sems = refs[-1]
    copies = []
    at = 0
    for src, dst, cut in zip(refs[:count], refs[count : 2 * count], pieces):
        for piece in range(cut):
            a, b = (src.at[piece], dst.at[piece]) if cut > 1 else (src, dst)
            copies.append(pltpu.make_async_copy(a, b, sems.at[at]))
            at += 1
    for copy in copies:
        copy.start()
    for copy in copies:
        copy.wait()


def put(arrays, pieces):
    return pl.pallas_call(
        functools.partial(put_kernel, len(arrays), pieces),
        out_shape=[jax.ShapeDtypeStruct(a.shape, a.dtype) for a in arrays],
        in_specs=[vmem] * len(arrays),
        out_specs=[hbm] * len(arrays),
        scratch_shapes=[DMA((sum(pieces),))],
        compiler_params=pltpu.CompilerParams(vmem_limit_bytes=16 * 1024 * 1024),
    )(*arrays)


def body(
    n, m, tokens, norm_gain, query_weight, key_weight, value_weight, outgate_weight,
    ingate_weight, forget_weight, forget_bias, output_weight, state_memory, state_normaliser,
    state_stabiliser, past_keys, past_values, past_ingate, past_forget, accepted,
):
    outs = cell(
        n, m, tokens, norm_gain[None, :], ingate_weight.T, forget_weight.T,
        forget_bias[None, :], (query_weight, key_weight, value_weight, outgate_weight),
        output_weight, state_memory, state_normaliser, state_stabiliser.T, past_keys,
        past_values, past_ingate.transpose(1, 2, 0), past_forget.transpose(1, 2, 0),
        accepted[None, :],
    )
    mixed, keys, values, memory, normaliser, stabiliser = put(
        outs, (1, 1, 1, state_memory.shape[0], 1, 1)
    )
    return (mixed, memory, normaliser, stabiliser.T, keys, values)


def solution(mesh):
    rows = P("kv", "tp")
    chained = P("kv", None, "tp")
    return jax.shard_map(
        functools.partial(body, mesh.shape["kv"], mesh.shape["tp"]),
        mesh=mesh,
        in_specs=(
            rows, P(), rows, rows, rows, rows, P(), P(), P(), P("tp", "kv"),
            P("kv", "tp", None, None), P("kv", "tp", None), rows,
            chained, chained, chained, chained, P("kv"),
        ),
        out_specs=(
            rows, P("kv", "tp", None, None), P("kv", "tp", None), rows, rows, rows,
        ),
        check_vma=False,
    )
```

```python
import functools

import jax
import jax.numpy as jnp
from jax import lax
from jax.experimental import pallas as pl
from jax.experimental.pallas import tpu as pltpu
from jax.sharding import PartitionSpec as P

epsilon = 1e-06
MESH = pl.DeviceIdType.MESH
vmem = pl.BlockSpec(memory_space=pltpu.VMEM)
hbm = pl.BlockSpec(memory_space=pltpu.HBM)
f32 = jnp.float32
bf16 = jnp.bfloat16
DMA = pltpu.SemaphoreType.DMA


def signal(sem, kv, tp):
    pl.semaphore_signal(sem, inc=1, device_id={"kv": kv, "tp": tp}, device_id_type=MESH)


def remote(src, dst, send_sem, recv_sem, kv, tp):
    return pltpu.make_async_remote_copy(
        src_ref=src,
        dst_ref=dst,
        send_sem=send_sem,
        recv_sem=recv_sem,
        device_id={"kv": kv, "tp": tp},
        device_id_type=MESH,
    )


def each(count, step, start=0):
    def run(index, carry):
        step(index)
        return carry

    lax.fori_loop(start, count, run, 0)


def log_sigmoid(v):
    return jnp.minimum(v, 0.0) - jnp.log1p(jnp.exp(-jnp.abs(v)))


def iota(shape, axis):
    return lax.broadcasted_iota(jnp.int32, shape, axis)


def cell_kernel(
    n, m, all_heads, features, chain,
    tok_h, gain_h, wi_h, wf_h, bias_h, w0_h, w1_h, w2_h, w3_h, wo_h,
    memory_h, norm_h, stab_h, past_k_h, past_v_h, past_i_h, past_f_h, taken_h,
    mixed, key_b, value_b, memory, norm_new, stab_new,
    tok, gain, wg, bias, w_in, w_out, norm, stab, past_k, past_v, past_i, past_f, taken,
    x_buf, xs, keep, give, near, pair, far, total_c, g_own, g_buf,
    m_low, weights, decay, spread, carries, query_b, outgate_b, from_memory, gated,
    a_buf, p_buf, q_buf, o_send, o_buf,
    in_sem, w_sem, m_sem, t_send, f_send, x_recv, g_send, g_recv,
    n_send, n_recv, z_send, z_recv, a_send, a_recv, p_send, p_recv, o_ssem, o_rsem,
):
    k = lax.axis_index("kv")
    t = lax.axis_index("tp")
    r = n // m
    half = n // 2
    pairs = m // 2
    rows, local = tok.shape
    width = xs.shape[2]
    cols = w_in.shape[2]
    out_cols = w_out.shape[1]
    seqs, heads, dk, dv = memory.shape
    z = k // 2
    x = k % 2
    core = t % 2
    partner = t + 1 - 2 * core
    beside = z * 2 + 1 - x
    t0 = k // r
    mine = k % r
    root = t0 == t
    root_core = t0 % 2 == core
    turn = 1 - 2 * (z // max(half // 2, 1))

    upper = z // max(half // 2, 1)

    def flip(p):
        return p + upper * (half - 1 - 2 * p)

    def plane(i):
        return lax.rem(z + i * turn + half, half)

    def order(i):
        past = (i + flip(z)) // half
        return flip((half - i) * (1 - past) + (i + flip(z) - half) * past)

    def slot_of(p):
        below = (flip(p) < flip(z)).astype(jnp.int32)
        return (half - flip(p)) * (1 - below) + (flip(p) + half - flip(z)) * below

    small = [
        pltpu.make_async_copy(tok_h, tok, in_sem.at[0]),
        pltpu.make_async_copy(gain_h, gain, in_sem.at[1]),
        pltpu.make_async_copy(
            wi_h.at[:, pl.ds(pl.multiple_of(t * local, local), local)],
            wg.at[pl.ds(0, all_heads)], in_sem.at[2],
        ),
        pltpu.make_async_copy(
            wf_h.at[:, pl.ds(pl.multiple_of(t * local, local), local)],
            wg.at[pl.ds(all_heads, all_heads)], in_sem.at[3],
        ),
    ]
    late = [
        pltpu.make_async_copy(src, dst, in_sem.at[4 + i])
        for i, (src, dst) in enumerate((
            (bias_h, bias), (norm_h, norm), (stab_h, stab), (past_k_h, past_k),
            (past_v_h, past_v), (past_i_h, past_i), (past_f_h, past_f), (taken_h, taken),
        ))
    ]
    big = [
        pltpu.make_async_copy(src, w_in.at[i], w_sem.at[min(i, 1)])
        for i, src in enumerate((w0_h, w1_h, w2_h, w3_h))
    ]
    load_out = pltpu.make_async_copy(wo_h, w_out, w_sem.at[2])

    def load(q):
        return pltpu.make_async_copy(memory_h.at[q], memory.at[q], m_sem)

    for copy in small + big + late:
        copy.start()
    load_out.start()
    each(seqs, lambda q: load(q).start())

    barrier = pltpu.get_barrier_semaphore()
    each(n, lambda i: signal(barrier, lax.rem(k + i, n), t), 1)
    each(m, lambda j: signal(barrier, k, lax.rem(t + j, m)), 1)
    split = m // 2

    def sum_place(kb):
        return (kb % 2) * split + (kb // 2) % split

    def sum_block(j):
        return 2 * (j * split + t % split) + t // split

    last_at = sum_place(k)

    def greet_root(h):
        @pl.when(jnp.logical_and(h != mine, jnp.logical_not(root)))
        def _():
            signal(barrier, t0 * r + h, t0)

    each(r, greet_root)

    def greet_last(h):
        kk = t * r + h

        @pl.when(jnp.logical_not(jnp.logical_and(kk == k, last_at == t)))
        def _():
            signal(barrier, kk, last_at)

    each(r, greet_last)
    both = jnp.logical_and(root, last_at == t).astype(jnp.int32)
    pl.semaphore_wait(
        barrier,
        (n - 1) + (m - 1) + r - both + root.astype(jnp.int32) * (r - 1) * (m - 1),
    )

    small[0].wait()

    def cut(h):
        return pl.ds(pl.multiple_of(h * width, width), width)

    def token_copy(h):
        return remote(
            tok.at[:, cut(h)], x_buf.at[k], t_send, x_recv.at[k], t * r + h, t
        )

    def group_copy(h, tt):
        return remote(
            tok.at[:, cut(h)], x_buf.at[k], t_send, x_recv.at[k], t0 * r + h, tt
        )

    def group_each(act):
        def at_place(h):
            def to_tp(j):
                tt = lax.rem(t + j, m)

                @pl.when(jnp.logical_not(jnp.logical_and(h == mine, j == 0)))
                def _():
                    act(group_copy(h, tt))

            each(m, to_tp)

        each(r, at_place)

    @pl.when(root)
    def _():
        group_each(lambda copy: copy.start())
        x_buf[k] = tok[:, cut(mine)]

    @pl.when(jnp.logical_not(root))
    def _():
        each(r, lambda h: token_copy(h).start())

    def forward(j, i, to):
        return remote(x_buf.at[j], x_buf.at[j], f_send.at[i], x_recv.at[j], k, to)

    def cousin(i):
        return lax.rem(t + 2 * i, m)

    def routed(j, act):
        outside = j // r != t0

        @pl.when(jnp.logical_and(root, outside))
        def _():
            for i in range(1, pairs):
                act(forward(j, i, cousin(i)))

        @pl.when(jnp.logical_and(root_core, outside))
        def _():
            act(forward(j, 0, partner))

    def pass_token(j):
        @pl.when(jnp.logical_not(jnp.logical_and(root, j == k)))
        def _():
            remote(
                tok.at[:, pl.ds(0, width)], x_buf.at[j], t_send, x_recv.at[j], k, t
            ).wait_recv()

        routed(j, lambda copy: copy.start())

    wg[pl.ds(2 * all_heads, wg.shape[0] - 2 * all_heads), :] = jnp.zeros(
        (wg.shape[0] - 2 * all_heads, local), bf16
    )
    for copy in small[1:]:
        copy.wait()
    floats = tok[...].astype(f32)
    squares = jnp.sum(floats * floats, axis=1, keepdims=True)
    lifted = floats * gain[:, pl.ds(pl.multiple_of(t * local, local), local)]
    raw = lax.dot_general(
        lifted.astype(bf16), wg[...], (((1,), (1,)), ((), ())), preferred_element_type=f32
    )
    lane = iota(raw.shape, 1)
    g_own[...] = jnp.where(lane < 2 * all_heads, raw, squares)

    def gate_copy(j):
        return remote(
            g_own, g_buf.at[j - 1], g_send, g_recv, k, lax.rem(t + j, m)
        )

    each(m, lambda j: gate_copy(j).start(), 1)
    own_gain = gain[:, pl.ds(pl.multiple_of(k * width, width), width)]

    def near_copy(c, i):
        return remote(give.at[c, i], near.at[c, i], n_send, n_recv.at[c, i], beside, t)

    def project(c, start, stop):
        both = xs[start:stop].reshape((stop - start) * 2 * rows, width)
        part = jnp.dot(both, w_in[c], preferred_element_type=f32).astype(bf16)
        for i in range(start, stop):
            at = (i - start) * 2 * rows
            give[c, i] = part[at : at + rows]
            keep[c, i] = part[at + rows : at + 2 * rows]

    def take_plane(p, i):
        for side, j in enumerate((p * 2 + 1 - x, p * 2 + x)):
            pass_token(j)
            xs[i, side * rows : (side + 1) * rows, :] = (
                x_buf[j].astype(f32) * own_gain
            ).astype(bf16)

    take_plane(z, 0)
    big[0].wait()
    project(0, 0, 1)
    near_copy(0, 0).start()
    pltpu.make_async_copy(w_in.at[pl.ds(1, 3)], w_in.at[pl.ds(1, 3)], w_sem.at[1]).wait()
    project(1, 0, 1)
    near_copy(1, 0).start()

    def far_plane(i):
        p = plane(i)
        take_plane(p, slot_of(p))

    each(half, far_plane, 1)
    project(0, 1, half)
    each(half, lambda i: near_copy(0, i).start(), 1)
    for c in range(1, 4):
        project(c, 1, half)

    def start_near(i):
        for c in range(1, 4):
            near_copy(c, i).start()

    each(half, start_near, 1)
    for c in range(2, 4):
        project(c, 0, 1)
        near_copy(c, 0).start()

    for copy in late:
        copy.wait()
    key_scale = dk ** (-0.5)
    reach = taken[...]
    chain_sum = jnp.zeros((heads, seqs), f32)
    running = []
    for j in range(chain):
        chain_sum = chain_sum + jnp.where(j < reach, log_sigmoid(past_f[j]), 0.0)
        running.append(chain_sum)
    carried_log = chain_sum + stab[...]
    new_stab = carried_log
    ends = []
    for j in range(chain):
        ends.append(jnp.where(j < reach, chain_sum - running[j] + past_i[j], -jnp.inf))
        new_stab = jnp.maximum(new_stab, ends[j])
    stab_new[...] = new_stab
    decay[...] = jnp.exp(carried_log - new_stab)
    for j in range(chain):
        weight_j = jnp.exp(ends[j] - new_stab)
        for h in range(heads):
            weights[h, j : j + 1, :] = weight_j[h : h + 1, :]

    remote(g_buf, g_buf, g_send, g_recv, k, t).wait_recv()
    total = g_own[...]
    for j in range(m - 1):
        total = total + g_buf[j]
    scale = lax.rsqrt(total[:, 2 * all_heads : 2 * all_heads + 1] / features + epsilon)
    gates = total * scale

    token_row = iota((rows, rows), 0)
    token_col = iota((rows, rows), 1)
    same_seq = token_row // chain == token_col // chain
    causal = jnp.logical_and(same_seq, token_col <= token_row)
    diagonal = token_row == token_col
    own_seq = iota((rows, seqs), 0) // chain == iota((rows, seqs), 1)
    first = t * heads

    def to_row(col):
        return jnp.sum(jnp.where(diagonal, col, 0.0), axis=0, keepdims=True)

    def pick(array, at):
        return jnp.sum(
            jnp.where(iota(array.shape, 1) == at, array, 0.0), axis=1, keepdims=True
        )

    for h in range(heads):
        in_col = pick(gates, first + h)
        forget = pick(gates, all_heads + first + h) + pick(bias[...], first + h)
        b_col = jnp.sum(
            jnp.where(causal, to_row(log_sigmoid(forget)), 0.0), axis=1, keepdims=True
        )
        within = jnp.where(causal, b_col + to_row(in_col - b_col), -jnp.inf)
        stab_col = jnp.sum(
            jnp.where(own_seq, stab_new[h : h + 1, :], 0.0), axis=1, keepdims=True
        )
        carried = b_col + stab_col
        stable = jnp.maximum(carried, jnp.max(within, axis=1, keepdims=True))
        spread[h] = jnp.exp(within - stable) * key_scale
        carries[h] = jnp.broadcast_to(jnp.exp(carried - stable), carries.shape[1:])

    def take(q):
        for h in range(heads):
            at = slice(h * dk, (h + 1) * dk)
            w_col = jnp.sum(
                jnp.where(iota((chain, seqs), 1) == q, weights[h], 0.0), axis=1, keepdims=True
            )
            fade = jnp.sum(
                jnp.where(iota((1, seqs), 1) == q, decay[h : h + 1, :], 0.0),
                axis=1, keepdims=True,
            )
            lifted_k = past_k[q, :, at].astype(f32) * key_scale * w_col
            norm_new[q, h : h + 1, :] = fade * norm[q, h : h + 1, :] + jnp.sum(
                lifted_k, axis=0, keepdims=True
            )
            added = lax.dot_general(
                lifted_k.astype(bf16),
                past_v[q, :, h * dv : (h + 1) * dv],
                (((0,), (0,)), ((), ())),
                preferred_element_type=f32,
            )
            new = fade * memory[q, h] + added
            memory[q, h] = new
            m_low[q, h] = new.astype(bf16)

    def line_copy(c, i):
        p = order(i)
        left = (p < z).astype(jnp.int32)
        slot = p + (p == z - 1).astype(jnp.int32) * (half - p)
        return remote(
            pair.at[c, i - 1], far.at[c, slot], z_send, z_recv.at[c, slot],
            (z + 1 - 2 * left) * 2 + x, t,
        )

    def line_wait(c, slot):
        remote(
            pair.at[c, 0], far.at[c, slot], z_send, z_recv.at[c, slot], k, t
        ).wait_recv()

    def fold(c, i):
        p = order(i)
        near_copy(c, i).wait_recv()
        starts = jnp.logical_or(
            jnp.logical_and(p > z, z == 0), jnp.logical_and(p < z, z == half - 1)
        )

        @pl.when(starts)
        def _():
            pair[c, i - 1] = (keep[c, i].astype(f32) + near[c, i].astype(f32)).astype(bf16)

        @pl.when(jnp.logical_not(starts))
        def _():
            line_wait(c, p)
            pair[c, i - 1] = (
                keep[c, i].astype(f32) + near[c, i].astype(f32) + far[c, p].astype(f32)
            ).astype(bf16)

        line_copy(c, i).start()

    pltpu.make_async_copy(memory_h, memory, m_sem).wait()

    def fold_query(i):
        fold(0, i)
        each(seqs * i // (half - 1), take, seqs * (i - 1) // (half - 1))

    each(half, fold_query, 1)

    def fold_rest(i):
        for c in range(1, 4):
            fold(c, i)

    each(half, fold_rest, 1)

    def settle(c, out):
        near_copy(c, 0).wait_recv()
        total_c[...] = keep[c, 0].astype(f32) + near[c, 0].astype(f32)

        def add(slot):
            line_wait(c, slot)
            total_c[...] += far[c, slot].astype(f32)

        @pl.when(z > 0)
        def _():
            add(z)

        @pl.when(z < half - 1)
        def _():
            add(half)

        out[...] = (total_c[...] * scale).astype(bf16)

    settle(0, query_b)
    row_seq = iota((rows, dv), 0) // chain
    from_memory[...] = jnp.zeros(from_memory.shape, f32)

    def recall(q):
        for h in range(heads):
            at = slice(h * dv, (h + 1) * dv)
            got = jnp.dot(
                query_b[:, h * dk : (h + 1) * dk], m_low[q, h], preferred_element_type=f32
            )
            from_memory[:, at] = jnp.where(row_seq == q, got, from_memory[:, at])

    each(seqs, recall)
    settle(1, key_b)

    scores, dens = [], []
    for h in range(heads):
        at = slice(h * dk, (h + 1) * dk)
        match = lax.dot_general(
            query_b[:, at], key_b[:, at], (((1,), (1,)), ((), ())), preferred_element_type=f32
        )
        score = match * spread[h]
        across_n = lax.dot_general(
            query_b[:, at].astype(f32), norm_new[:, h, :], (((1,), (1,)), ((), ())),
            precision=lax.Precision.HIGHEST, preferred_element_type=f32,
        )
        q_n = jnp.sum(jnp.where(own_seq, across_n, 0.0), axis=1, keepdims=True)
        den = carries[h, :, :1] * q_n + jnp.sum(score, axis=1, keepdims=True)
        scores.append(score.astype(bf16))
        dens.append(1.0 / jnp.maximum(jnp.abs(den), 1.0))

    settle(2, value_b)
    for h in range(heads):
        at = slice(h * dv, (h + 1) * dv)
        fresh = jnp.dot(scores[h], value_b[:, at], preferred_element_type=f32)
        from_memory[:, at] = (carries[h, :, :1] * from_memory[:, at] + fresh) * dens[h]
    settle(3, outgate_b)
    gated[...] = (jax.nn.sigmoid(outgate_b[...].astype(f32)) * from_memory[...]).astype(bf16)

    def along_copy(i):
        return remote(gated, a_buf.at[k], a_send, a_recv.at[k], plane(i) * 2 + x, t)

    def across_copy(i):
        at = plane(i) * 2 + x
        return remote(a_buf.at[at], a_buf.at[at], a_send, a_recv.at[at], beside, t)

    own_copy = remote(gated, a_buf.at[k], a_send, a_recv.at[k], beside, t)
    each(half, lambda i: along_copy(i).start(), 1)
    own_copy.start()
    a_buf[k] = gated[...]
    load_out.wait()

    def landed(at):
        remote(gated, a_buf.at[at], a_send, a_recv.at[at], k, t).wait_recv()

    def part_copy(kb):
        j = kb // m
        return remote(
            p_buf.at[kb], q_buf.at[j, t], p_send, p_recv.at[j, t], k, sum_place(kb)
        )

    def away(kb):
        return sum_place(kb) != t

    def mix_plane(p):
        landed(p * 2 + 1 - x)
        both_rows = a_buf[pl.ds(p * 2, 2)].reshape(2 * rows, cols)
        part = jnp.dot(both_rows, w_out[...], preferred_element_type=f32).astype(bf16)
        for side in range(2):
            kb = p * 2 + side
            p_buf[kb] = part[side * rows : (side + 1) * rows]

            @pl.when(away(kb))
            def _():
                part_copy(kb).start()

    def step_plane(i):
        landed(plane(i) * 2 + x)
        across_copy(i).start()
        mix_plane(plane(i - 1))

    each(half, step_plane, 1)
    mix_plane(plane(half - 1))

    def final_copy(j):
        return remote(
            o_send.at[j], o_buf.at[mine], o_ssem.at[j], o_rsem.at[mine], sum_block(j), t0
        )

    def stays(j):
        return jnp.logical_and(root, sum_block(j) == k)

    for j in range(r):
        def landed_part(tt, j=j):
            @pl.when(tt != t)
            def _():
                remote(
                    p_buf.at[0], q_buf.at[j, tt], p_send, p_recv.at[j, tt], k, t
                ).wait_recv()

        each(m, landed_part)
        q_buf[j, t] = p_buf[sum_block(j)]
        summed = q_buf[j, 0].astype(f32)
        for tt in range(1, m):
            summed = summed + q_buf[j, tt].astype(f32)
        o_send[j] = summed.astype(bf16)

        @pl.when(jnp.logical_not(stays(j)))
        def _(j=j):
            final_copy(j).start()

        @pl.when(stays(j))
        def _(j=j):
            o_buf[mine] = o_send[j]

    for h in range(r):
        @pl.when(jnp.logical_not(jnp.logical_and(t * r + h == k, last_at == t)))
        def _(h=h):
            remote(
                o_send.at[0], o_buf.at[h], o_ssem.at[0], o_rsem.at[h], k, t
            ).wait_recv()

        mixed[:, h * out_cols : (h + 1) * out_cols] = o_buf[h]

    @pl.when(root)
    def _():
        sent = x_buf.at[pl.ds(0, n - 1)]
        remote(sent, sent, t_send, x_recv.at[0], k, t).wait_send()
        for i in range(1, pairs):
            sent = x_buf.at[pl.ds(0, n - r)]
            remote(sent, sent, f_send.at[i], x_recv.at[0], k, t).wait_send()

    @pl.when(jnp.logical_not(root))
    def _():
        remote(tok, tok, t_send, x_recv.at[0], k, t).wait_send()

    @pl.when(root_core)
    def _():
        sent = x_buf.at[pl.ds(0, n - r)]
        remote(sent, sent, f_send.at[0], x_recv.at[0], k, t).wait_send()

    remote(g_buf, g_buf, g_send, g_recv, k, t).wait_send()
    remote(give, give, n_send, n_recv.at[0, 0], k, t).wait_send()
    remote(pair, pair, z_send, z_recv.at[0, 0], k, t).wait_send()
    sent = a_buf.at[pl.ds(0, n - 1)]
    remote(sent, sent, a_send, a_recv.at[0], k, t).wait_send()
    sent = p_buf.at[pl.ds(0, n - r)]
    remote(sent, sent, p_send, p_recv.at[0, 0], k, t).wait_send()
    for j in range(r):
        @pl.when(jnp.logical_not(stays(j)))
        def _(j=j):
            final_copy(j).wait_send()


def cell(n, m, tokens, gain, wi, wf, bias, weights, w_out, memory, norm, stab, past_k, past_v,
         past_i, past_f, taken):
    seqs, heads, dk, dv = memory.shape
    rows, local = tokens.shape
    width, cols = weights[0].shape
    all_heads = wi.shape[0]
    chain = past_k.shape[1]
    depth, out_cols = w_out.shape
    half, r = n // 2, n // m
    lanes = -(-(2 * all_heads + 1) // 128) * 128
    V = pltpu.VMEM
    outs = [
        V((rows, local), bf16), V((rows, cols), bf16), V((rows, cols), bf16),
        V(memory.shape, f32), V(norm.shape, f32), V(stab.shape, f32),
    ]
    return pl.pallas_call(
        functools.partial(cell_kernel, n, m, all_heads, local * m, chain),
        out_shape=outs,
        in_specs=[hbm] * 18,
        out_specs=[vmem] * 6,
        scratch_shapes=[
            V((rows, local), bf16), V(gain.shape, f32), V((lanes, local), bf16),
            V(bias.shape, f32), V((4, width, cols), bf16), V(w_out.shape, bf16),
            V(norm.shape, f32), V(stab.shape, f32), V(past_k.shape, bf16),
            V(past_v.shape, bf16), V(past_i.shape, f32), V(past_f.shape, f32),
            V(taken.shape, jnp.int32),
            V((n, rows, width), bf16), V((half, 2 * rows, width), bf16),
            V((4, half, rows, cols), bf16), V((4, half, rows, cols), bf16),
            V((4, half, rows, cols), bf16), V((4, half - 1, rows, cols), bf16),
            V((4, half + 1, rows, cols), bf16), V((rows, cols), f32),
            V((rows, lanes), f32), V((m - 1, rows, lanes), f32),
            V(memory.shape, bf16), V((heads, chain, seqs), f32), V(stab.shape, f32),
            V((heads, rows, rows), f32), V((heads, rows, 128), f32),
            V((rows, cols), bf16), V((rows, cols), bf16), V((rows, cols), f32),
            V((rows, cols), bf16),
            V((n, rows, cols), bf16), V((n, rows, out_cols), bf16),
            V((r, m, rows, out_cols), bf16), V((r, rows, out_cols), bf16),
            V((r, rows, out_cols), bf16),
            DMA((12,)), DMA((3,)), DMA, DMA, DMA((m // 2,)), DMA((n,)), DMA, DMA,
            DMA, DMA((4, half)), DMA, DMA((4, half + 1)),
            DMA, DMA((n,)), DMA, DMA((r, m)), DMA((r,)), DMA((r,)),
        ],
        compiler_params=pltpu.CompilerParams(
            collective_id=0, has_side_effects=True, vmem_limit_bytes=40 * 1024 * 1024
        ),
    )(*(pltpu.with_memory_space_constraint(a, pltpu.HBM) for a in (
        tokens, gain, wi, wf, bias, *weights, w_out, memory, norm, stab, past_k, past_v,
        past_i, past_f, taken,
    )))


def put_kernel(count, pieces, *refs):
    sems = refs[-1]
    copies = []
    at = 0
    for src, dst, cut in zip(refs[:count], refs[count : 2 * count], pieces):
        for piece in range(cut):
            a, b = (src.at[piece], dst.at[piece]) if cut > 1 else (src, dst)
            copies.append(pltpu.make_async_copy(a, b, sems.at[at]))
            at += 1
    for copy in copies:
        copy.start()
    for copy in copies:
        copy.wait()


def put(arrays, pieces):
    return pl.pallas_call(
        functools.partial(put_kernel, len(arrays), pieces),
        out_shape=[jax.ShapeDtypeStruct(a.shape, a.dtype) for a in arrays],
        in_specs=[vmem] * len(arrays),
        out_specs=[hbm] * len(arrays),
        scratch_shapes=[DMA((sum(pieces),))],
        compiler_params=pltpu.CompilerParams(vmem_limit_bytes=16 * 1024 * 1024),
    )(*arrays)


def body(
    n, m, tokens, norm_gain, query_weight, key_weight, value_weight, outgate_weight,
    ingate_weight, forget_weight, forget_bias, output_weight, state_memory, state_normaliser,
    state_stabiliser, past_keys, past_values, past_ingate, past_forget, accepted,
):
    outs = cell(
        n, m, tokens, norm_gain[None, :], ingate_weight.T, forget_weight.T,
        forget_bias[None, :], (query_weight, key_weight, value_weight, outgate_weight),
        output_weight, state_memory, state_normaliser, state_stabiliser.T, past_keys,
        past_values, past_ingate.transpose(1, 2, 0), past_forget.transpose(1, 2, 0),
        accepted[None, :],
    )
    mixed, keys, values, memory, normaliser, stabiliser = put(
        outs, (1, 1, 1, state_memory.shape[0], 1, 1)
    )
    return (mixed, memory, normaliser, stabiliser.T, keys, values)


def solution(mesh):
    rows = P("kv", "tp")
    chained = P("kv", None, "tp")
    return jax.shard_map(
        functools.partial(body, mesh.shape["kv"], mesh.shape["tp"]),
        mesh=mesh,
        in_specs=(
            rows, P(), rows, rows, rows, rows, P(), P(), P(), P("tp", "kv"),
            P("kv", "tp", None, None), P("kv", "tp", None), rows,
            chained, chained, chained, chained, P("kv"),
        ),
        out_specs=(
            rows, P("kv", "tp", None, None), P("kv", "tp", None), rows, rows, rows,
        ),
        check_vma=False,
    )
```

```python
import functools

import jax
import jax.numpy as jnp
from jax import lax
from jax.experimental import pallas as pl
from jax.experimental.pallas import tpu as pltpu
from jax.sharding import PartitionSpec as P

epsilon = 1e-06
MESH = pl.DeviceIdType.MESH
vmem = pl.BlockSpec(memory_space=pltpu.VMEM)
hbm = pl.BlockSpec(memory_space=pltpu.HBM)
f32 = jnp.float32
bf16 = jnp.bfloat16
DMA = pltpu.SemaphoreType.DMA


def signal(sem, kv, tp):
    pl.semaphore_signal(sem, inc=1, device_id={"kv": kv, "tp": tp}, device_id_type=MESH)


def remote(src, dst, send_sem, recv_sem, kv, tp):
    return pltpu.make_async_remote_copy(
        src_ref=src,
        dst_ref=dst,
        send_sem=send_sem,
        recv_sem=recv_sem,
        device_id={"kv": kv, "tp": tp},
        device_id_type=MESH,
    )


def each(count, step, start=0):
    def run(index, carry):
        step(index)
        return carry

    lax.fori_loop(start, count, run, 0)


def log_sigmoid(v):
    return jnp.minimum(v, 0.0) - jnp.log1p(jnp.exp(-jnp.abs(v)))


def iota(shape, axis):
    return lax.broadcasted_iota(jnp.int32, shape, axis)


def cell_kernel(
    n, m, all_heads, features, chain,
    tok_h, gain_h, wi_h, wf_h, bias_h, w0_h, w1_h, w2_h, w3_h, wo_h,
    memory_h, norm_h, stab_h, past_k_h, past_v_h, past_i_h, past_f_h, taken_h,
    mixed, key_b, value_b, memory, norm_new, stab_new,
    tok, gain, wg, bias, w_in, w_out, norm, stab, past_k, past_v, past_i, past_f, taken,
    x_buf, xs, keep, give, near, pair, far, total_c, g_own, g_buf,
    m_low, weights, decay, spread, carries, query_b, outgate_b, from_memory, gated,
    a_buf, p_buf, q_buf, o_send, o_buf,
    in_sem, w_sem, m_sem, t_send, f_send, x_recv, g_send, g_recv,
    n_send, n_recv, z_send, z_recv, a_send, a_recv, p_send, p_recv, o_ssem, o_rsem,
):
    k = lax.axis_index("kv")
    t = lax.axis_index("tp")
    r = n // m
    half = n // 2
    pairs = m // 2
    rows, local = tok.shape
    width = xs.shape[2]
    cols = w_in.shape[2]
    out_cols = w_out.shape[1]
    seqs, heads, dk, dv = memory.shape
    z = k // 2
    x = k % 2
    core = t % 2
    partner = t + 1 - 2 * core
    beside = z * 2 + 1 - x
    t0 = k // r
    mine = k % r
    root = t0 == t
    root_core = t0 % 2 == core

    upper = z // max(half // 2, 1)

    def flip(p):
        return p + upper * (half - 1 - 2 * p)

    def plane(i):
        at = flip(z)
        back = jnp.int32(half) - i
        right = half - 1 - at
        first = (back < right).astype(jnp.int32)
        last = (back == half - 1).astype(jnp.int32)
        return flip(
            first * (1 - last) * i
            + (1 - first) * (1 - last) * (back - right)
            + last * (at + 1)
        )

    def order(i):
        past = (i + flip(z)) // half
        return flip((half - i) * (1 - past) + (i + flip(z) - half) * past)

    def slot_of(p):
        below = (flip(p) < flip(z)).astype(jnp.int32)
        return (half - flip(p)) * (1 - below) + (flip(p) + half - flip(z)) * below

    small = [
        pltpu.make_async_copy(tok_h, tok, in_sem.at[0]),
        pltpu.make_async_copy(gain_h, gain, in_sem.at[1]),
        pltpu.make_async_copy(
            wi_h.at[:, pl.ds(pl.multiple_of(t * local, local), local)],
            wg.at[pl.ds(0, all_heads)], in_sem.at[2],
        ),
        pltpu.make_async_copy(
            wf_h.at[:, pl.ds(pl.multiple_of(t * local, local), local)],
            wg.at[pl.ds(all_heads, all_heads)], in_sem.at[3],
        ),
    ]
    late = [
        pltpu.make_async_copy(src, dst, in_sem.at[4 + i])
        for i, (src, dst) in enumerate((
            (bias_h, bias), (norm_h, norm), (stab_h, stab), (past_k_h, past_k),
            (past_v_h, past_v), (past_i_h, past_i), (past_f_h, past_f), (taken_h, taken),
        ))
    ]
    big = [
        pltpu.make_async_copy(src, w_in.at[i], w_sem.at[min(i, 1)])
        for i, src in enumerate((w0_h, w1_h, w2_h, w3_h))
    ]
    load_out = pltpu.make_async_copy(wo_h, w_out, w_sem.at[2])

    def load(q):
        return pltpu.make_async_copy(memory_h.at[q], memory.at[q], m_sem)

    for copy in small + big + late:
        copy.start()
    load_out.start()
    each(seqs, lambda q: load(q).start())

    barrier = pltpu.get_barrier_semaphore()
    each(n, lambda i: signal(barrier, lax.rem(k + i, n), t), 1)
    each(m, lambda j: signal(barrier, k, lax.rem(t + j, m)), 1)
    split = m // 2

    def sum_place(kb):
        return (kb % 2) * split + (kb // 2) % split

    def sum_block(j):
        return 2 * (j * split + t % split) + t // split

    last_at = sum_place(k)

    def greet_root(h):
        @pl.when(jnp.logical_and(h != mine, jnp.logical_not(root)))
        def _():
            signal(barrier, t0 * r + h, t0)

    each(r, greet_root)

    @pl.when(jnp.logical_and(root_core, jnp.logical_not(root)))
    def _():
        def greet_source(j):
            @pl.when(j // r != t0)
            def _():
                signal(barrier, j, t0)

        each(n, greet_source)


    def greet_last(h):
        kk = t * r + h

        @pl.when(jnp.logical_not(jnp.logical_and(kk == k, last_at == t)))
        def _():
            signal(barrier, kk, last_at)

    each(r, greet_last)
    both = jnp.logical_and(root, last_at == t).astype(jnp.int32)
    pl.semaphore_wait(
        barrier,
        (n - 1) + (m - 1) + r - both
        + root.astype(jnp.int32) * ((r - 1) * (m - 1) - r * (pairs - 1))
        + r * (pairs - 1),
    )

    small[0].wait()

    def cousin(i):
        return lax.rem(t + 2 * i, m)

    def cut(h):
        return pl.ds(pl.multiple_of(h * width, width), width)

    def token_copy(h, i):
        return remote(
            tok.at[:, cut(h)], x_buf.at[k], t_send, x_recv.at[k], t * r + h, cousin(i)
        )

    def group_copy(h, tt):
        return remote(
            tok.at[:, cut(h)], x_buf.at[k], t_send, x_recv.at[k], t0 * r + h, tt
        )

    def group_each(act):
        def at_place(h):
            def to_tp(j):
                tt = lax.rem(t + j, m)

                @pl.when(jnp.logical_not(jnp.logical_and(h == mine, j == 0)))
                def _():
                    act(group_copy(h, tt))

            each(m, to_tp)

        each(r, at_place)

    @pl.when(root)
    def _():
        group_each(lambda copy: copy.start())
        x_buf[k] = tok[:, cut(mine)]

    @pl.when(jnp.logical_not(root))
    def _():
        for i in range(pairs):
            each(r, lambda h, i=i: token_copy(h, i).start())

    def forward(j):
        return remote(x_buf.at[j], x_buf.at[j], f_send, x_recv.at[j], k, partner)

    def pass_token(j):
        @pl.when(jnp.logical_not(jnp.logical_and(root, j == k)))
        def _():
            remote(
                tok.at[:, pl.ds(0, width)], x_buf.at[j], t_send, x_recv.at[j], k, t
            ).wait_recv()

        @pl.when(jnp.logical_and(root_core, j // r != t0))
        def _():
            forward(j).start()

    wg[pl.ds(2 * all_heads, wg.shape[0] - 2 * all_heads), :] = jnp.zeros(
        (wg.shape[0] - 2 * all_heads, local), bf16
    )
    for copy in small[1:]:
        copy.wait()
    floats = tok[...].astype(f32)
    squares = jnp.sum(floats * floats, axis=1, keepdims=True)
    lifted = floats * gain[:, pl.ds(pl.multiple_of(t * local, local), local)]
    raw = lax.dot_general(
        lifted.astype(bf16), wg[...], (((1,), (1,)), ((), ())), preferred_element_type=f32
    )
    lane = iota(raw.shape, 1)
    g_own[...] = jnp.where(lane < 2 * all_heads, raw, squares)

    def gate_copy(j):
        return remote(
            g_own, g_buf.at[j - 1], g_send, g_recv, k, lax.rem(t + j, m)
        )

    each(m, lambda j: gate_copy(j).start(), 1)
    own_gain = gain[:, pl.ds(pl.multiple_of(k * width, width), width)]

    def near_copy(c, i):
        return remote(give.at[c, i], near.at[c, i], n_send, n_recv.at[c, i], beside, t)

    def project(c, start, stop):
        both = xs[start:stop].reshape((stop - start) * 2 * rows, width)
        part = jnp.dot(both, w_in[c], preferred_element_type=f32).astype(bf16)
        for i in range(start, stop):
            at = (i - start) * 2 * rows
            give[c, i] = part[at : at + rows]
            keep[c, i] = part[at + rows : at + 2 * rows]

    def take_plane(p, i):
        for side, j in enumerate((p * 2 + 1 - x, p * 2 + x)):
            pass_token(j)
            xs[i, side * rows : (side + 1) * rows, :] = (
                x_buf[j].astype(f32) * own_gain
            ).astype(bf16)

    take_plane(z, 0)
    big[0].wait()
    project(0, 0, 1)
    near_copy(0, 0).start()
    pltpu.make_async_copy(w_in.at[pl.ds(1, 3)], w_in.at[pl.ds(1, 3)], w_sem.at[1]).wait()
    project(1, 0, 1)
    near_copy(1, 0).start()

    def far_plane(i):
        p = plane(i)
        take_plane(p, slot_of(p))

    each(half, far_plane, 1)
    project(0, 1, half)
    each(half, lambda i: near_copy(0, i).start(), 1)
    for c in range(1, 4):
        project(c, 1, half)

    def start_near(i):
        for c in range(1, 4):
            near_copy(c, i).start()

    each(half, start_near, 1)
    for c in range(2, 4):
        project(c, 0, 1)
        near_copy(c, 0).start()

    for copy in late:
        copy.wait()
    key_scale = dk ** (-0.5)
    reach = taken[...]
    chain_sum = jnp.zeros((heads, seqs), f32)
    running = []
    for j in range(chain):
        chain_sum = chain_sum + jnp.where(j < reach, log_sigmoid(past_f[j]), 0.0)
        running.append(chain_sum)
    carried_log = chain_sum + stab[...]
    new_stab = carried_log
    ends = []
    for j in range(chain):
        ends.append(jnp.where(j < reach, chain_sum - running[j] + past_i[j], -jnp.inf))
        new_stab = jnp.maximum(new_stab, ends[j])
    stab_new[...] = new_stab
    decay[...] = jnp.exp(carried_log - new_stab)
    for j in range(chain):
        weight_j = jnp.exp(ends[j] - new_stab)
        for h in range(heads):
            weights[h, j : j + 1, :] = weight_j[h : h + 1, :]

    remote(g_buf, g_buf, g_send, g_recv, k, t).wait_recv()
    total = g_own[...]
    for j in range(m - 1):
        total = total + g_buf[j]
    scale = lax.rsqrt(total[:, 2 * all_heads : 2 * all_heads + 1] / features + epsilon)
    gates = total * scale

    token_row = iota((rows, rows), 0)
    token_col = iota((rows, rows), 1)
    same_seq = token_row // chain == token_col // chain
    causal = jnp.logical_and(same_seq, token_col <= token_row)
    diagonal = token_row == token_col
    own_seq = iota((rows, seqs), 0) // chain == iota((rows, seqs), 1)
    first = t * heads

    def to_row(col):
        return jnp.sum(jnp.where(diagonal, col, 0.0), axis=0, keepdims=True)

    def pick(array, at):
        return jnp.sum(
            jnp.where(iota(array.shape, 1) == at, array, 0.0), axis=1, keepdims=True
        )

    for h in range(heads):
        in_col = pick(gates, first + h)
        forget = pick(gates, all_heads + first + h) + pick(bias[...], first + h)
        b_col = jnp.sum(
            jnp.where(causal, to_row(log_sigmoid(forget)), 0.0), axis=1, keepdims=True
        )
        within = jnp.where(causal, b_col + to_row(in_col - b_col), -jnp.inf)
        stab_col = jnp.sum(
            jnp.where(own_seq, stab_new[h : h + 1, :], 0.0), axis=1, keepdims=True
        )
        carried = b_col + stab_col
        stable = jnp.maximum(carried, jnp.max(within, axis=1, keepdims=True))
        spread[h] = jnp.exp(within - stable) * key_scale
        carries[h] = jnp.broadcast_to(jnp.exp(carried - stable), carries.shape[1:])

    def take(q):
        for h in range(heads):
            at = slice(h * dk, (h + 1) * dk)
            w_col = jnp.sum(
                jnp.where(iota((chain, seqs), 1) == q, weights[h], 0.0), axis=1, keepdims=True
            )
            fade = jnp.sum(
                jnp.where(iota((1, seqs), 1) == q, decay[h : h + 1, :], 0.0),
                axis=1, keepdims=True,
            )
            lifted_k = past_k[q, :, at].astype(f32) * key_scale * w_col
            norm_new[q, h : h + 1, :] = fade * norm[q, h : h + 1, :] + jnp.sum(
                lifted_k, axis=0, keepdims=True
            )
            added = lax.dot_general(
                lifted_k.astype(bf16),
                past_v[q, :, h * dv : (h + 1) * dv],
                (((0,), (0,)), ((), ())),
                preferred_element_type=f32,
            )
            new = fade * memory[q, h] + added
            memory[q, h] = new
            m_low[q, h] = new.astype(bf16)

    def line_copy(c, i):
        p = order(i)
        left = (p < z).astype(jnp.int32)
        slot = p + (p == z - 1).astype(jnp.int32) * (half - p)
        return remote(
            pair.at[c, i - 1], far.at[c, slot], z_send, z_recv.at[c, slot],
            (z + 1 - 2 * left) * 2 + x, t,
        )

    def line_wait(c, slot):
        remote(
            pair.at[c, 0], far.at[c, slot], z_send, z_recv.at[c, slot], k, t
        ).wait_recv()

    def fold(c, i):
        p = order(i)
        near_copy(c, i).wait_recv()
        starts = jnp.logical_or(
            jnp.logical_and(p > z, z == 0), jnp.logical_and(p < z, z == half - 1)
        )

        @pl.when(starts)
        def _():
            pair[c, i - 1] = (keep[c, i].astype(f32) + near[c, i].astype(f32)).astype(bf16)

        @pl.when(jnp.logical_not(starts))
        def _():
            line_wait(c, p)
            pair[c, i - 1] = (
                keep[c, i].astype(f32) + near[c, i].astype(f32) + far[c, p].astype(f32)
            ).astype(bf16)

        line_copy(c, i).start()

    pltpu.make_async_copy(memory_h, memory, m_sem).wait()

    def fold_query(i):
        fold(0, i)
        each(seqs * i // (half - 1), take, seqs * (i - 1) // (half - 1))

    each(half, fold_query, 1)

    def fold_rest(i):
        for c in range(1, 4):
            fold(c, i)

    each(half, fold_rest, 1)

    def settle(c, out):
        near_copy(c, 0).wait_recv()
        total_c[...] = keep[c, 0].astype(f32) + near[c, 0].astype(f32)

        def add(slot):
            line_wait(c, slot)
            total_c[...] += far[c, slot].astype(f32)

        @pl.when(z > 0)
        def _():
            add(z)

        @pl.when(z < half - 1)
        def _():
            add(half)

        out[...] = (total_c[...] * scale).astype(bf16)

    settle(0, query_b)
    row_seq = iota((rows, dv), 0) // chain
    from_memory[...] = jnp.zeros(from_memory.shape, f32)

    def recall(q):
        for h in range(heads):
            at = slice(h * dv, (h + 1) * dv)
            got = jnp.dot(
                query_b[:, h * dk : (h + 1) * dk], m_low[q, h], preferred_element_type=f32
            )
            from_memory[:, at] = jnp.where(row_seq == q, got, from_memory[:, at])

    each(seqs, recall)
    settle(1, key_b)

    scores, dens = [], []
    for h in range(heads):
        at = slice(h * dk, (h + 1) * dk)
        match = lax.dot_general(
            query_b[:, at], key_b[:, at], (((1,), (1,)), ((), ())), preferred_element_type=f32
        )
        score = match * spread[h]
        across_n = lax.dot_general(
            query_b[:, at].astype(f32), norm_new[:, h, :], (((1,), (1,)), ((), ())),
            precision=lax.Precision.HIGHEST, preferred_element_type=f32,
        )
        q_n = jnp.sum(jnp.where(own_seq, across_n, 0.0), axis=1, keepdims=True)
        den = carries[h, :, :1] * q_n + jnp.sum(score, axis=1, keepdims=True)
        scores.append(score.astype(bf16))
        dens.append(1.0 / jnp.maximum(jnp.abs(den), 1.0))

    settle(2, value_b)
    for h in range(heads):
        at = slice(h * dv, (h + 1) * dv)
        fresh = jnp.dot(scores[h], value_b[:, at], preferred_element_type=f32)
        from_memory[:, at] = (carries[h, :, :1] * from_memory[:, at] + fresh) * dens[h]
    settle(3, outgate_b)
    gated[...] = (jax.nn.sigmoid(outgate_b[...].astype(f32)) * from_memory[...]).astype(bf16)

    def along_copy(i):
        return remote(gated, a_buf.at[k], a_send, a_recv.at[k], plane(i) * 2 + x, t)

    def across_copy(i):
        at = plane(i) * 2 + x
        return remote(a_buf.at[at], a_buf.at[at], a_send, a_recv.at[at], beside, t)

    own_copy = remote(gated, a_buf.at[k], a_send, a_recv.at[k], beside, t)
    each(half, lambda i: along_copy(i).start(), 1)
    own_copy.start()
    a_buf[k] = gated[...]
    load_out.wait()

    def landed(at):
        remote(gated, a_buf.at[at], a_send, a_recv.at[at], k, t).wait_recv()

    def part_copy(kb):
        j = kb // m
        return remote(
            p_buf.at[kb], q_buf.at[j, t], p_send, p_recv.at[j, t], k, sum_place(kb)
        )

    def away(kb):
        return sum_place(kb) != t

    def mix_plane(p):
        landed(p * 2 + 1 - x)
        both_rows = a_buf[pl.ds(p * 2, 2)].reshape(2 * rows, cols)
        part = jnp.dot(both_rows, w_out[...], preferred_element_type=f32).astype(bf16)
        for side in range(2):
            kb = p * 2 + side
            p_buf[kb] = part[side * rows : (side + 1) * rows]

            @pl.when(away(kb))
            def _():
                part_copy(kb).start()

    def pass_on(i):
        landed(plane(i) * 2 + x)
        across_copy(i).start()

    each(half, pass_on, 1)
    mix_plane(z)
    each(half - 1, lambda i: mix_plane(plane(i)), 1)
    mix_plane(plane(half - 1))

    def final_copy(j):
        return remote(
            o_send.at[j], o_buf.at[mine], o_ssem.at[j], o_rsem.at[mine], sum_block(j), t0
        )

    def stays(j):
        return jnp.logical_and(root, sum_block(j) == k)

    for j in range(r):
        def landed_part(tt, j=j):
            @pl.when(tt != t)
            def _():
                remote(
                    p_buf.at[0], q_buf.at[j, tt], p_send, p_recv.at[j, tt], k, t
                ).wait_recv()

        each(m, landed_part)
        q_buf[j, t] = p_buf[sum_block(j)]
        summed = q_buf[j, 0].astype(f32)
        for tt in range(1, m):
            summed = summed + q_buf[j, tt].astype(f32)
        o_send[j] = summed.astype(bf16)

        @pl.when(jnp.logical_not(stays(j)))
        def _(j=j):
            final_copy(j).start()

        @pl.when(stays(j))
        def _(j=j):
            o_buf[mine] = o_send[j]

    for h in range(r):
        @pl.when(jnp.logical_not(jnp.logical_and(t * r + h == k, last_at == t)))
        def _(h=h):
            remote(
                o_send.at[0], o_buf.at[h], o_ssem.at[0], o_rsem.at[h], k, t
            ).wait_recv()

        mixed[:, h * out_cols : (h + 1) * out_cols] = o_buf[h]

    @pl.when(root)
    def _():
        sent = x_buf.at[pl.ds(0, n - 1)]
        remote(sent, sent, t_send, x_recv.at[0], k, t).wait_send()

    @pl.when(jnp.logical_not(root))
    def _():
        sent = x_buf.at[pl.ds(0, r * pairs)]
        remote(sent, sent, t_send, x_recv.at[0], k, t).wait_send()

    @pl.when(root_core)
    def _():
        sent = x_buf.at[pl.ds(0, n - r)]
        remote(sent, sent, f_send, x_recv.at[0], k, t).wait_send()

    remote(g_buf, g_buf, g_send, g_recv, k, t).wait_send()
    remote(give, give, n_send, n_recv.at[0, 0], k, t).wait_send()
    remote(pair, pair, z_send, z_recv.at[0, 0], k, t).wait_send()
    sent = a_buf.at[pl.ds(0, n - 1)]
    remote(sent, sent, a_send, a_recv.at[0], k, t).wait_send()
    sent = p_buf.at[pl.ds(0, n - r)]
    remote(sent, sent, p_send, p_recv.at[0, 0], k, t).wait_send()
    for j in range(r):
        @pl.when(jnp.logical_not(stays(j)))
        def _(j=j):
            final_copy(j).wait_send()


def cell(n, m, tokens, gain, wi, wf, bias, weights, w_out, memory, norm, stab, past_k, past_v,
         past_i, past_f, taken):
    seqs, heads, dk, dv = memory.shape
    rows, local = tokens.shape
    width, cols = weights[0].shape
    all_heads = wi.shape[0]
    chain = past_k.shape[1]
    depth, out_cols = w_out.shape
    half, r = n // 2, n // m
    lanes = -(-(2 * all_heads + 1) // 128) * 128
    V = pltpu.VMEM
    outs = [
        V((rows, local), bf16), V((rows, cols), bf16), V((rows, cols), bf16),
        V(memory.shape, f32), V(norm.shape, f32), V(stab.shape, f32),
    ]
    return pl.pallas_call(
        functools.partial(cell_kernel, n, m, all_heads, local * m, chain),
        out_shape=outs,
        in_specs=[hbm] * 18,
        out_specs=[vmem] * 6,
        scratch_shapes=[
            V((rows, local), bf16), V(gain.shape, f32), V((lanes, local), bf16),
            V(bias.shape, f32), V((4, width, cols), bf16), V(w_out.shape, bf16),
            V(norm.shape, f32), V(stab.shape, f32), V(past_k.shape, bf16),
            V(past_v.shape, bf16), V(past_i.shape, f32), V(past_f.shape, f32),
            V(taken.shape, jnp.int32),
            V((n, rows, width), bf16), V((half, 2 * rows, width), bf16),
            V((4, half, rows, cols), bf16), V((4, half, rows, cols), bf16),
            V((4, half, rows, cols), bf16), V((4, half - 1, rows, cols), bf16),
            V((4, half + 1, rows, cols), bf16), V((rows, cols), f32),
            V((rows, lanes), f32), V((m - 1, rows, lanes), f32),
            V(memory.shape, bf16), V((heads, chain, seqs), f32), V(stab.shape, f32),
            V((heads, rows, rows), f32), V((heads, rows, 128), f32),
            V((rows, cols), bf16), V((rows, cols), bf16), V((rows, cols), f32),
            V((rows, cols), bf16),
            V((n, rows, cols), bf16), V((n, rows, out_cols), bf16),
            V((r, m, rows, out_cols), bf16), V((r, rows, out_cols), bf16),
            V((r, rows, out_cols), bf16),
            DMA((12,)), DMA((3,)), DMA, DMA, DMA, DMA((n,)), DMA, DMA,
            DMA, DMA((4, half)), DMA, DMA((4, half + 1)),
            DMA, DMA((n,)), DMA, DMA((r, m)), DMA((r,)), DMA((r,)),
        ],
        compiler_params=pltpu.CompilerParams(
            collective_id=0, has_side_effects=True, vmem_limit_bytes=40 * 1024 * 1024
        ),
    )(*(pltpu.with_memory_space_constraint(a, pltpu.HBM) for a in (
        tokens, gain, wi, wf, bias, *weights, w_out, memory, norm, stab, past_k, past_v,
        past_i, past_f, taken,
    )))


def put_kernel(count, pieces, *refs):
    sems = refs[-1]
    copies = []
    at = 0
    for src, dst, cut in zip(refs[:count], refs[count : 2 * count], pieces):
        for piece in range(cut):
            a, b = (src.at[piece], dst.at[piece]) if cut > 1 else (src, dst)
            copies.append(pltpu.make_async_copy(a, b, sems.at[at]))
            at += 1
    for copy in copies:
        copy.start()
    for copy in copies:
        copy.wait()


def put(arrays, pieces):
    return pl.pallas_call(
        functools.partial(put_kernel, len(arrays), pieces),
        out_shape=[jax.ShapeDtypeStruct(a.shape, a.dtype) for a in arrays],
        in_specs=[vmem] * len(arrays),
        out_specs=[hbm] * len(arrays),
        scratch_shapes=[DMA((sum(pieces),))],
        compiler_params=pltpu.CompilerParams(vmem_limit_bytes=16 * 1024 * 1024),
    )(*arrays)


def body(
    n, m, tokens, norm_gain, query_weight, key_weight, value_weight, outgate_weight,
    ingate_weight, forget_weight, forget_bias, output_weight, state_memory, state_normaliser,
    state_stabiliser, past_keys, past_values, past_ingate, past_forget, accepted,
):
    outs = cell(
        n, m, tokens, norm_gain[None, :], ingate_weight.T, forget_weight.T,
        forget_bias[None, :], (query_weight, key_weight, value_weight, outgate_weight),
        output_weight, state_memory, state_normaliser, state_stabiliser.T, past_keys,
        past_values, past_ingate.transpose(1, 2, 0), past_forget.transpose(1, 2, 0),
        accepted[None, :],
    )
    mixed, keys, values, memory, normaliser, stabiliser = put(
        outs, (1, 1, 1, state_memory.shape[0], 1, 1)
    )
    return (mixed, memory, normaliser, stabiliser.T, keys, values)


def solution(mesh):
    rows = P("kv", "tp")
    chained = P("kv", None, "tp")
    return jax.shard_map(
        functools.partial(body, mesh.shape["kv"], mesh.shape["tp"]),
        mesh=mesh,
        in_specs=(
            rows, P(), rows, rows, rows, rows, P(), P(), P(), P("tp", "kv"),
            P("kv", "tp", None, None), P("kv", "tp", None), rows,
            chained, chained, chained, chained, P("kv"),
        ),
        out_specs=(
            rows, P("kv", "tp", None, None), P("kv", "tp", None), rows, rows, rows,
        ),
        check_vma=False,
    )
```

```python
import functools

import jax
import jax.numpy as jnp
from jax import lax
from jax.experimental import pallas as pl
from jax.experimental.pallas import tpu as pltpu
from jax.sharding import PartitionSpec as P

epsilon = 1e-06
MESH = pl.DeviceIdType.MESH
vmem = pl.BlockSpec(memory_space=pltpu.VMEM)
hbm = pl.BlockSpec(memory_space=pltpu.HBM)
f32 = jnp.float32
bf16 = jnp.bfloat16
DMA = pltpu.SemaphoreType.DMA


def signal(sem, kv, tp):
    pl.semaphore_signal(sem, inc=1, device_id={"kv": kv, "tp": tp}, device_id_type=MESH)


def remote(src, dst, send_sem, recv_sem, kv, tp):
    return pltpu.make_async_remote_copy(
        src_ref=src,
        dst_ref=dst,
        send_sem=send_sem,
        recv_sem=recv_sem,
        device_id={"kv": kv, "tp": tp},
        device_id_type=MESH,
    )


def each(count, step, start=0):
    def run(index, carry):
        step(index)
        return carry

    lax.fori_loop(start, count, run, 0)


def log_sigmoid(v):
    return jnp.minimum(v, 0.0) - jnp.log1p(jnp.exp(-jnp.abs(v)))


def iota(shape, axis):
    return lax.broadcasted_iota(jnp.int32, shape, axis)


def cell_kernel(
    n, m, all_heads, features, chain,
    tok_h, gain_h, wi_h, wf_h, bias_h, w0_h, w1_h, w2_h, w3_h, wo_h,
    memory_h, norm_h, stab_h, past_k_h, past_v_h, past_i_h, past_f_h, taken_h,
    mixed, key_b, value_b, memory, norm_new, stab_new,
    tok, gain, wg, bias, w_in, w_out, norm, stab, past_k, past_v, past_i, past_f, taken,
    x_buf, xs, keep, give, near, pair, far, total_c, g_own, g_buf,
    m_low, weights, decay, spread, carries, query_b, outgate_b, from_memory, gated,
    a_buf, p_buf, q_buf, o_send, o_buf,
    in_sem, w_sem, m_sem, t_send, f_send, x_recv, g_send, g_recv,
    n_send, n_recv, z_send, z_recv, a_send, a_recv, p_send, p_recv, o_ssem, o_rsem,
):
    k = lax.axis_index("kv")
    t = lax.axis_index("tp")
    r = n // m
    half = n // 2
    pairs = m // 2
    rows, local = tok.shape
    width = xs.shape[2]
    cols = w_in.shape[2]
    out_cols = w_out.shape[1]
    seqs, heads, dk, dv = memory.shape
    z = k // 2
    x = k % 2
    core = t % 2
    partner = t + 1 - 2 * core
    beside = z * 2 + 1 - x
    t0 = k // r
    mine = k % r
    root = t0 == t
    root_core = t0 % 2 == core

    upper = z // max(half // 2, 1)

    def flip(p):
        return p + upper * (half - 1 - 2 * p)

    def plane(i):
        at = flip(z)
        back = jnp.int32(half) - i
        right = half - 1 - at
        first = (back < right).astype(jnp.int32)
        last = (back == half - 1).astype(jnp.int32)
        return flip(
            first * (1 - last) * i
            + (1 - first) * (1 - last) * (back - right)
            + last * (at + 1)
        )

    def order(i):
        past = (i + flip(z)) // half
        return flip((half - i) * (1 - past) + (i + flip(z) - half) * past)

    def slot_of(p):
        below = (flip(p) < flip(z)).astype(jnp.int32)
        return (half - flip(p)) * (1 - below) + (flip(p) + half - flip(z)) * below

    small = [
        pltpu.make_async_copy(tok_h, tok, in_sem.at[0]),
        pltpu.make_async_copy(gain_h, gain, in_sem.at[1]),
        pltpu.make_async_copy(
            wi_h.at[:, pl.ds(pl.multiple_of(t * local, local), local)],
            wg.at[pl.ds(0, all_heads)], in_sem.at[2],
        ),
        pltpu.make_async_copy(
            wf_h.at[:, pl.ds(pl.multiple_of(t * local, local), local)],
            wg.at[pl.ds(all_heads, all_heads)], in_sem.at[3],
        ),
    ]
    late = [
        pltpu.make_async_copy(src, dst, in_sem.at[4 + i])
        for i, (src, dst) in enumerate((
            (bias_h, bias), (norm_h, norm), (stab_h, stab), (past_k_h, past_k),
            (past_v_h, past_v), (past_i_h, past_i), (past_f_h, past_f), (taken_h, taken),
        ))
    ]
    big = [
        pltpu.make_async_copy(src, w_in.at[i], w_sem.at[min(i, 1)])
        for i, src in enumerate((w0_h, w1_h, w2_h, w3_h))
    ]
    load_out = pltpu.make_async_copy(wo_h, w_out, w_sem.at[2])

    def load(q):
        return pltpu.make_async_copy(memory_h.at[q], memory.at[q], m_sem)

    for copy in small + big + late:
        copy.start()
    load_out.start()
    each(seqs, lambda q: load(q).start())

    barrier = pltpu.get_barrier_semaphore()
    each(n, lambda i: signal(barrier, lax.rem(k + i, n), t), 1)
    each(m, lambda j: signal(barrier, k, lax.rem(t + j, m)), 1)
    def pair_core(y):
        return 2 * y + k % 2

    def is_me(kk, tt):
        return jnp.logical_and(kk == k, tt == t)

    def greet_root(h):
        @pl.when(jnp.logical_and(h != mine, jnp.logical_not(root)))
        def _():
            signal(barrier, t0 * r + h, t0)

    each(r, greet_root)

    @pl.when(jnp.logical_and(root_core, jnp.logical_not(root)))
    def _():
        def greet_source(j):
            @pl.when(j // r != t0)
            def _():
                signal(barrier, j, t0)

        each(n, greet_source)


    def greet_last(h):
        for y in range(pairs):
            @pl.when(jnp.logical_not(is_me(t * r + h, pair_core(y))))
            def _(y=y):
                signal(barrier, t * r + h, pair_core(y))

    each(r, greet_last)
    both = jnp.logical_and(root, k % 2 == core).astype(jnp.int32)
    pl.semaphore_wait(
        barrier,
        (n - 1) + (m - 1) + half - both
        + root.astype(jnp.int32) * ((r - 1) * (m - 1) - r * (pairs - 1))
        + r * (pairs - 1),
    )

    small[0].wait()

    def cousin(i):
        return lax.rem(t + 2 * i, m)

    def cut(h):
        return pl.ds(pl.multiple_of(h * width, width), width)

    def token_copy(h, i):
        return remote(
            tok.at[:, cut(h)], x_buf.at[k], t_send, x_recv.at[k], t * r + h, cousin(i)
        )

    def group_copy(h, tt):
        return remote(
            tok.at[:, cut(h)], x_buf.at[k], t_send, x_recv.at[k], t0 * r + h, tt
        )

    def group_each(act):
        def at_place(h):
            def to_tp(j):
                tt = lax.rem(t + j, m)

                @pl.when(jnp.logical_not(jnp.logical_and(h == mine, j == 0)))
                def _():
                    act(group_copy(h, tt))

            each(m, to_tp)

        each(r, at_place)

    @pl.when(root)
    def _():
        group_each(lambda copy: copy.start())
        x_buf[k] = tok[:, cut(mine)]

    @pl.when(jnp.logical_not(root))
    def _():
        for i in range(pairs):
            each(r, lambda h, i=i: token_copy(h, i).start())

    def forward(j):
        return remote(x_buf.at[j], x_buf.at[j], f_send, x_recv.at[j], k, partner)

    def pass_token(j):
        @pl.when(jnp.logical_not(jnp.logical_and(root, j == k)))
        def _():
            remote(
                tok.at[:, pl.ds(0, width)], x_buf.at[j], t_send, x_recv.at[j], k, t
            ).wait_recv()

        @pl.when(jnp.logical_and(root_core, j // r != t0))
        def _():
            forward(j).start()

    wg[pl.ds(2 * all_heads, wg.shape[0] - 2 * all_heads), :] = jnp.zeros(
        (wg.shape[0] - 2 * all_heads, local), bf16
    )
    for copy in small[1:]:
        copy.wait()
    floats = tok[...].astype(f32)
    squares = jnp.sum(floats * floats, axis=1, keepdims=True)
    lifted = floats * gain[:, pl.ds(pl.multiple_of(t * local, local), local)]
    raw = lax.dot_general(
        lifted.astype(bf16), wg[...], (((1,), (1,)), ((), ())), preferred_element_type=f32
    )
    lane = iota(raw.shape, 1)
    g_own[...] = jnp.where(lane < 2 * all_heads, raw, squares)

    def gate_copy(j):
        return remote(
            g_own, g_buf.at[j - 1], g_send, g_recv, k, lax.rem(t + j, m)
        )

    each(m, lambda j: gate_copy(j).start(), 1)
    own_gain = gain[:, pl.ds(pl.multiple_of(k * width, width), width)]

    def near_copy(c, i):
        return remote(give.at[c, i], near.at[c, i], n_send, n_recv.at[c, i], beside, t)

    def project(c, start, stop):
        both = xs[start:stop].reshape((stop - start) * 2 * rows, width)
        part = jnp.dot(both, w_in[c], preferred_element_type=f32).astype(bf16)
        for i in range(start, stop):
            at = (i - start) * 2 * rows
            give[c, i] = part[at : at + rows]
            keep[c, i] = part[at + rows : at + 2 * rows]

    def take_plane(p, i):
        for side, j in enumerate((p * 2 + 1 - x, p * 2 + x)):
            pass_token(j)
            xs[i, side * rows : (side + 1) * rows, :] = (
                x_buf[j].astype(f32) * own_gain
            ).astype(bf16)

    take_plane(z, 0)
    big[0].wait()
    project(0, 0, 1)
    near_copy(0, 0).start()
    pltpu.make_async_copy(w_in.at[pl.ds(1, 3)], w_in.at[pl.ds(1, 3)], w_sem.at[1]).wait()
    project(1, 0, 1)
    near_copy(1, 0).start()

    def far_plane(i):
        p = plane(i)
        take_plane(p, slot_of(p))

    each(half, far_plane, 1)
    project(0, 1, half)
    each(half, lambda i: near_copy(0, i).start(), 1)
    for c in range(1, 4):
        project(c, 1, half)

    def start_near(i):
        for c in range(1, 4):
            near_copy(c, i).start()

    each(half, start_near, 1)
    for c in range(2, 4):
        project(c, 0, 1)
        near_copy(c, 0).start()

    for copy in late:
        copy.wait()
    key_scale = dk ** (-0.5)
    reach = taken[...]
    chain_sum = jnp.zeros((heads, seqs), f32)
    running = []
    for j in range(chain):
        chain_sum = chain_sum + jnp.where(j < reach, log_sigmoid(past_f[j]), 0.0)
        running.append(chain_sum)
    carried_log = chain_sum + stab[...]
    new_stab = carried_log
    ends = []
    for j in range(chain):
        ends.append(jnp.where(j < reach, chain_sum - running[j] + past_i[j], -jnp.inf))
        new_stab = jnp.maximum(new_stab, ends[j])
    stab_new[...] = new_stab
    decay[...] = jnp.exp(carried_log - new_stab)
    for j in range(chain):
        weight_j = jnp.exp(ends[j] - new_stab)
        for h in range(heads):
            weights[h, j : j + 1, :] = weight_j[h : h + 1, :]

    remote(g_buf, g_buf, g_send, g_recv, k, t).wait_recv()
    total = g_own[...]
    for j in range(m - 1):
        total = total + g_buf[j]
    scale = lax.rsqrt(total[:, 2 * all_heads : 2 * all_heads + 1] / features + epsilon)
    gates = total * scale

    token_row = iota((rows, rows), 0)
    token_col = iota((rows, rows), 1)
    same_seq = token_row // chain == token_col // chain
    causal = jnp.logical_and(same_seq, token_col <= token_row)
    diagonal = token_row == token_col
    own_seq = iota((rows, seqs), 0) // chain == iota((rows, seqs), 1)
    first = t * heads

    def to_row(col):
        return jnp.sum(jnp.where(diagonal, col, 0.0), axis=0, keepdims=True)

    def pick(array, at):
        return jnp.sum(
            jnp.where(iota(array.shape, 1) == at, array, 0.0), axis=1, keepdims=True
        )

    for h in range(heads):
        in_col = pick(gates, first + h)
        forget = pick(gates, all_heads + first + h) + pick(bias[...], first + h)
        b_col = jnp.sum(
            jnp.where(causal, to_row(log_sigmoid(forget)), 0.0), axis=1, keepdims=True
        )
        within = jnp.where(causal, b_col + to_row(in_col - b_col), -jnp.inf)
        stab_col = jnp.sum(
            jnp.where(own_seq, stab_new[h : h + 1, :], 0.0), axis=1, keepdims=True
        )
        carried = b_col + stab_col
        stable = jnp.maximum(carried, jnp.max(within, axis=1, keepdims=True))
        spread[h] = jnp.exp(within - stable) * key_scale
        carries[h] = jnp.broadcast_to(jnp.exp(carried - stable), carries.shape[1:])

    def take(q):
        for h in range(heads):
            at = slice(h * dk, (h + 1) * dk)
            w_col = jnp.sum(
                jnp.where(iota((chain, seqs), 1) == q, weights[h], 0.0), axis=1, keepdims=True
            )
            fade = jnp.sum(
                jnp.where(iota((1, seqs), 1) == q, decay[h : h + 1, :], 0.0),
                axis=1, keepdims=True,
            )
            lifted_k = past_k[q, :, at].astype(f32) * key_scale * w_col
            norm_new[q, h : h + 1, :] = fade * norm[q, h : h + 1, :] + jnp.sum(
                lifted_k, axis=0, keepdims=True
            )
            added = lax.dot_general(
                lifted_k.astype(bf16),
                past_v[q, :, h * dv : (h + 1) * dv],
                (((0,), (0,)), ((), ())),
                preferred_element_type=f32,
            )
            new = fade * memory[q, h] + added
            memory[q, h] = new
            m_low[q, h] = new.astype(bf16)

    def line_copy(c, i):
        p = order(i)
        left = (p < z).astype(jnp.int32)
        slot = p + (p == z - 1).astype(jnp.int32) * (half - p)
        return remote(
            pair.at[c, i - 1], far.at[c, slot], z_send, z_recv.at[c, slot],
            (z + 1 - 2 * left) * 2 + x, t,
        )

    def line_wait(c, slot):
        remote(
            pair.at[c, 0], far.at[c, slot], z_send, z_recv.at[c, slot], k, t
        ).wait_recv()

    def fold(c, i):
        p = order(i)
        near_copy(c, i).wait_recv()
        starts = jnp.logical_or(
            jnp.logical_and(p > z, z == 0), jnp.logical_and(p < z, z == half - 1)
        )

        @pl.when(starts)
        def _():
            pair[c, i - 1] = (keep[c, i].astype(f32) + near[c, i].astype(f32)).astype(bf16)

        @pl.when(jnp.logical_not(starts))
        def _():
            line_wait(c, p)
            pair[c, i - 1] = (
                keep[c, i].astype(f32) + near[c, i].astype(f32) + far[c, p].astype(f32)
            ).astype(bf16)

        line_copy(c, i).start()

    pltpu.make_async_copy(memory_h, memory, m_sem).wait()

    def fold_query(i):
        fold(0, i)
        each(seqs * i // (half - 1), take, seqs * (i - 1) // (half - 1))

    each(half, fold_query, 1)

    def fold_rest(i):
        for c in range(1, 4):
            fold(c, i)

    each(half, fold_rest, 1)

    def settle(c, out):
        near_copy(c, 0).wait_recv()
        total_c[...] = keep[c, 0].astype(f32) + near[c, 0].astype(f32)

        def add(slot):
            line_wait(c, slot)
            total_c[...] += far[c, slot].astype(f32)

        @pl.when(z > 0)
        def _():
            add(z)

        @pl.when(z < half - 1)
        def _():
            add(half)

        out[...] = (total_c[...] * scale).astype(bf16)

    settle(0, query_b)
    row_seq = iota((rows, dv), 0) // chain
    from_memory[...] = jnp.zeros(from_memory.shape, f32)

    def recall(q):
        for h in range(heads):
            at = slice(h * dv, (h + 1) * dv)
            got = jnp.dot(
                query_b[:, h * dk : (h + 1) * dk], m_low[q, h], preferred_element_type=f32
            )
            from_memory[:, at] = jnp.where(row_seq == q, got, from_memory[:, at])

    each(seqs, recall)
    settle(1, key_b)

    scores, dens = [], []
    for h in range(heads):
        at = slice(h * dk, (h + 1) * dk)
        match = lax.dot_general(
            query_b[:, at], key_b[:, at], (((1,), (1,)), ((), ())), preferred_element_type=f32
        )
        score = match * spread[h]
        across_n = lax.dot_general(
            query_b[:, at].astype(f32), norm_new[:, h, :], (((1,), (1,)), ((), ())),
            precision=lax.Precision.HIGHEST, preferred_element_type=f32,
        )
        q_n = jnp.sum(jnp.where(own_seq, across_n, 0.0), axis=1, keepdims=True)
        den = carries[h, :, :1] * q_n + jnp.sum(score, axis=1, keepdims=True)
        scores.append(score.astype(bf16))
        dens.append(1.0 / jnp.maximum(jnp.abs(den), 1.0))

    settle(2, value_b)
    for h in range(heads):
        at = slice(h * dv, (h + 1) * dv)
        fresh = jnp.dot(scores[h], value_b[:, at], preferred_element_type=f32)
        from_memory[:, at] = (carries[h, :, :1] * from_memory[:, at] + fresh) * dens[h]
    settle(3, outgate_b)
    gated[...] = (jax.nn.sigmoid(outgate_b[...].astype(f32)) * from_memory[...]).astype(bf16)

    def along_copy(i):
        return remote(gated, a_buf.at[k], a_send, a_recv.at[k], plane(i) * 2 + x, t)

    def across_copy(i):
        at = plane(i) * 2 + x
        return remote(a_buf.at[at], a_buf.at[at], a_send, a_recv.at[at], beside, t)

    own_copy = remote(gated, a_buf.at[k], a_send, a_recv.at[k], beside, t)
    each(half, lambda i: along_copy(i).start(), 1)
    own_copy.start()
    a_buf[k] = gated[...]
    load_out.wait()

    def landed(at):
        remote(gated, a_buf.at[at], a_send, a_recv.at[at], k, t).wait_recv()

    def part_copy(p):
        return remote(
            p_buf.at[p * 2 + 1 - core], q_buf.at[p], p_send, p_recv.at[p], k, partner
        )

    def mix_plane(p):
        landed(p * 2 + 1 - x)
        both_rows = a_buf[pl.ds(p * 2, 2)].reshape(2 * rows, cols)
        part = jnp.dot(both_rows, w_out[...], preferred_element_type=f32).astype(bf16)
        for side in range(2):
            p_buf[p * 2 + side] = part[side * rows : (side + 1) * rows]
        part_copy(p).start()

    def final_copy(p):
        return remote(
            o_send.at[p], o_buf.at[mine, t // 2], o_ssem, o_rsem.at[mine, t // 2],
            p * 2 + core, t0,
        )

    def stays(p):
        return jnp.logical_and(root, p * 2 + core == k)

    def sum_plane(p):
        part_copy(p).wait_recv()
        o_send[p] = (
            p_buf[p * 2 + core].astype(f32) + q_buf[p].astype(f32)
        ).astype(bf16)

        @pl.when(jnp.logical_not(stays(p)))
        def _():
            final_copy(p).start()

        @pl.when(stays(p))
        def _():
            o_buf[mine, t // 2] = o_send[p]

    def pass_on(i):
        landed(plane(i) * 2 + x)
        across_copy(i).start()

    each(half, pass_on, 1)
    mix_plane(z)

    def mix_next(i):
        mix_plane(plane(i))
        later = (i > 1).astype(jnp.int32)
        sum_plane(later * plane(i - 1) + (1 - later) * z)

    each(half - 1, mix_next, 1)
    mix_plane(plane(half - 1))
    if half > 1:
        sum_plane(plane(half - 2))
    sum_plane(plane(half - 1))
    for h in range(r):
        for y in range(pairs):
            @pl.when(jnp.logical_not(is_me(t * r + h, pair_core(y))))
            def _(h=h, y=y):
                remote(
                    o_send.at[0], o_buf.at[h, y], o_ssem, o_rsem.at[h, y], k, t
                ).wait_recv()

        summed = o_buf[h, 0].astype(f32)
        for y in range(1, pairs):
            summed = summed + o_buf[h, y].astype(f32)
        mixed[:, h * out_cols : (h + 1) * out_cols] = summed.astype(bf16)

    @pl.when(root)
    def _():
        sent = x_buf.at[pl.ds(0, n - 1)]
        remote(sent, sent, t_send, x_recv.at[0], k, t).wait_send()

    @pl.when(jnp.logical_not(root))
    def _():
        sent = x_buf.at[pl.ds(0, r * pairs)]
        remote(sent, sent, t_send, x_recv.at[0], k, t).wait_send()

    @pl.when(root_core)
    def _():
        sent = x_buf.at[pl.ds(0, n - r)]
        remote(sent, sent, f_send, x_recv.at[0], k, t).wait_send()

    remote(g_buf, g_buf, g_send, g_recv, k, t).wait_send()
    remote(give, give, n_send, n_recv.at[0, 0], k, t).wait_send()
    remote(pair, pair, z_send, z_recv.at[0, 0], k, t).wait_send()
    sent = a_buf.at[pl.ds(0, n - 1)]
    remote(sent, sent, a_send, a_recv.at[0], k, t).wait_send()
    remote(q_buf, q_buf, p_send, p_recv.at[0], k, t).wait_send()
    keeps = jnp.logical_and(root, k % 2 == core)

    @pl.when(keeps)
    def _():
        sent = o_send.at[pl.ds(0, half - 1)]
        remote(sent, sent, o_ssem, o_rsem.at[0, 0], k, t).wait_send()

    @pl.when(jnp.logical_not(keeps))
    def _():
        remote(o_send, o_send, o_ssem, o_rsem.at[0, 0], k, t).wait_send()


def cell(n, m, tokens, gain, wi, wf, bias, weights, w_out, memory, norm, stab, past_k, past_v,
         past_i, past_f, taken):
    seqs, heads, dk, dv = memory.shape
    rows, local = tokens.shape
    width, cols = weights[0].shape
    all_heads = wi.shape[0]
    chain = past_k.shape[1]
    depth, out_cols = w_out.shape
    half, r = n // 2, n // m
    lanes = -(-(2 * all_heads + 1) // 128) * 128
    V = pltpu.VMEM
    outs = [
        V((rows, local), bf16), V((rows, cols), bf16), V((rows, cols), bf16),
        V(memory.shape, f32), V(norm.shape, f32), V(stab.shape, f32),
    ]
    return pl.pallas_call(
        functools.partial(cell_kernel, n, m, all_heads, local * m, chain),
        out_shape=outs,
        in_specs=[hbm] * 18,
        out_specs=[vmem] * 6,
        scratch_shapes=[
            V((rows, local), bf16), V(gain.shape, f32), V((lanes, local), bf16),
            V(bias.shape, f32), V((4, width, cols), bf16), V(w_out.shape, bf16),
            V(norm.shape, f32), V(stab.shape, f32), V(past_k.shape, bf16),
            V(past_v.shape, bf16), V(past_i.shape, f32), V(past_f.shape, f32),
            V(taken.shape, jnp.int32),
            V((n, rows, width), bf16), V((half, 2 * rows, width), bf16),
            V((4, half, rows, cols), bf16), V((4, half, rows, cols), bf16),
            V((4, half, rows, cols), bf16), V((4, half - 1, rows, cols), bf16),
            V((4, half + 1, rows, cols), bf16), V((rows, cols), f32),
            V((rows, lanes), f32), V((m - 1, rows, lanes), f32),
            V(memory.shape, bf16), V((heads, chain, seqs), f32), V(stab.shape, f32),
            V((heads, rows, rows), f32), V((heads, rows, 128), f32),
            V((rows, cols), bf16), V((rows, cols), bf16), V((rows, cols), f32),
            V((rows, cols), bf16),
            V((n, rows, cols), bf16), V((n, rows, out_cols), bf16),
            V((half, rows, out_cols), bf16), V((half, rows, out_cols), bf16),
            V((r, m // 2, rows, out_cols), bf16),
            DMA((12,)), DMA((3,)), DMA, DMA, DMA, DMA((n,)), DMA, DMA,
            DMA, DMA((4, half)), DMA, DMA((4, half + 1)),
            DMA, DMA((n,)), DMA, DMA((half,)), DMA, DMA((r, m // 2)),
        ],
        compiler_params=pltpu.CompilerParams(
            collective_id=0, has_side_effects=True, vmem_limit_bytes=40 * 1024 * 1024
        ),
    )(*(pltpu.with_memory_space_constraint(a, pltpu.HBM) for a in (
        tokens, gain, wi, wf, bias, *weights, w_out, memory, norm, stab, past_k, past_v,
        past_i, past_f, taken,
    )))


def put_kernel(count, pieces, *refs):
    sems = refs[-1]
    copies = []
    at = 0
    for src, dst, cut in zip(refs[:count], refs[count : 2 * count], pieces):
        for piece in range(cut):
            a, b = (src.at[piece], dst.at[piece]) if cut > 1 else (src, dst)
            copies.append(pltpu.make_async_copy(a, b, sems.at[at]))
            at += 1
    for copy in copies:
        copy.start()
    for copy in copies:
        copy.wait()


def put(arrays, pieces):
    return pl.pallas_call(
        functools.partial(put_kernel, len(arrays), pieces),
        out_shape=[jax.ShapeDtypeStruct(a.shape, a.dtype) for a in arrays],
        in_specs=[vmem] * len(arrays),
        out_specs=[hbm] * len(arrays),
        scratch_shapes=[DMA((sum(pieces),))],
        compiler_params=pltpu.CompilerParams(vmem_limit_bytes=16 * 1024 * 1024),
    )(*arrays)


def body(
    n, m, tokens, norm_gain, query_weight, key_weight, value_weight, outgate_weight,
    ingate_weight, forget_weight, forget_bias, output_weight, state_memory, state_normaliser,
    state_stabiliser, past_keys, past_values, past_ingate, past_forget, accepted,
):
    outs = cell(
        n, m, tokens, norm_gain[None, :], ingate_weight.T, forget_weight.T,
        forget_bias[None, :], (query_weight, key_weight, value_weight, outgate_weight),
        output_weight, state_memory, state_normaliser, state_stabiliser.T, past_keys,
        past_values, past_ingate.transpose(1, 2, 0), past_forget.transpose(1, 2, 0),
        accepted[None, :],
    )
    mixed, keys, values, memory, normaliser, stabiliser = put(
        outs, (1, 1, 1, state_memory.shape[0], 1, 1)
    )
    return (mixed, memory, normaliser, stabiliser.T, keys, values)


def solution(mesh):
    rows = P("kv", "tp")
    chained = P("kv", None, "tp")
    return jax.shard_map(
        functools.partial(body, mesh.shape["kv"], mesh.shape["tp"]),
        mesh=mesh,
        in_specs=(
            rows, P(), rows, rows, rows, rows, P(), P(), P(), P("tp", "kv"),
            P("kv", "tp", None, None), P("kv", "tp", None), rows,
            chained, chained, chained, chained, P("kv"),
        ),
        out_specs=(
            rows, P("kv", "tp", None, None), P("kv", "tp", None), rows, rows, rows,
        ),
        check_vma=False,
    )
```

```python
import functools

import jax
import jax.numpy as jnp
from jax import lax
from jax.experimental import pallas as pl
from jax.experimental.pallas import tpu as pltpu
from jax.sharding import PartitionSpec as P

epsilon = 1e-06
MESH = pl.DeviceIdType.MESH
vmem = pl.BlockSpec(memory_space=pltpu.VMEM)
hbm = pl.BlockSpec(memory_space=pltpu.HBM)
f32 = jnp.float32
bf16 = jnp.bfloat16
DMA = pltpu.SemaphoreType.DMA


def signal(sem, kv, tp):
    pl.semaphore_signal(sem, inc=1, device_id={"kv": kv, "tp": tp}, device_id_type=MESH)


def remote(src, dst, send_sem, recv_sem, kv, tp):
    return pltpu.make_async_remote_copy(
        src_ref=src,
        dst_ref=dst,
        send_sem=send_sem,
        recv_sem=recv_sem,
        device_id={"kv": kv, "tp": tp},
        device_id_type=MESH,
    )


def each(count, step, start=0):
    def run(index, carry):
        step(index)
        return carry

    lax.fori_loop(start, count, run, 0)


def log_sigmoid(v):
    return jnp.minimum(v, 0.0) - jnp.log1p(jnp.exp(-jnp.abs(v)))


def iota(shape, axis):
    return lax.broadcasted_iota(jnp.int32, shape, axis)


def cell_kernel(
    n, m, all_heads, features, chain,
    tok_h, gain_h, wi_h, wf_h, bias_h, w0_h, w1_h, w2_h, w3_h, wo_h,
    memory_h, norm_h, stab_h, past_k_h, past_v_h, past_i_h, past_f_h, taken_h,
    mixed, key_b, value_b, memory, norm_new, stab_new,
    tok, gain, wg, bias, w_in, w_out, norm, stab, past_k, past_v, past_i, past_f, taken,
    x_buf, xs, keep, give, near, pair, far, total_c, g_own, g_buf,
    m_low, weights, decay, spread, carries, query_b, outgate_b, from_memory, gated,
    a_buf, p_buf, q_buf, o_send, o_buf,
    in_sem, w_sem, m_sem, t_send, f_send, x_recv, g_send, g_recv,
    n_send, n_recv, z_send, z_recv, a_send, a_recv, p_send, p_recv, o_ssem, o_rsem,
):
    k = lax.axis_index("kv")
    t = lax.axis_index("tp")
    r = n // m
    half = n // 2
    pairs = m // 2
    rows, local = tok.shape
    width = xs.shape[2]
    cols = w_in.shape[2]
    out_cols = w_out.shape[1]
    seqs, heads, dk, dv = memory.shape
    z = k // 2
    x = k % 2
    core = t % 2
    partner = t + 1 - 2 * core
    beside = z * 2 + 1 - x
    t0 = k // r
    mine = k % r
    root = t0 == t
    root_core = t0 % 2 == core

    upper = z // max(half // 2, 1)

    def flip(p):
        return p + upper * (half - 1 - 2 * p)

    def plane(i):
        at = flip(z)
        back = jnp.int32(half) - i
        right = half - 1 - at
        first = (back < right).astype(jnp.int32)
        last = (back == half - 1).astype(jnp.int32)
        return flip(
            first * (1 - last) * i
            + (1 - first) * (1 - last) * (back - right)
            + last * (at + 1)
        )

    def order(i):
        past = (i + flip(z)) // half
        return flip((half - i) * (1 - past) + (i + flip(z) - half) * past)

    def slot_of(p):
        below = (flip(p) < flip(z)).astype(jnp.int32)
        return (half - flip(p)) * (1 - below) + (flip(p) + half - flip(z)) * below

    small = [
        pltpu.make_async_copy(tok_h, tok, in_sem.at[0]),
        pltpu.make_async_copy(gain_h, gain, in_sem.at[1]),
        pltpu.make_async_copy(
            wi_h.at[:, pl.ds(pl.multiple_of(t * local, local), local)],
            wg.at[pl.ds(0, all_heads)], in_sem.at[2],
        ),
        pltpu.make_async_copy(
            wf_h.at[:, pl.ds(pl.multiple_of(t * local, local), local)],
            wg.at[pl.ds(all_heads, all_heads)], in_sem.at[3],
        ),
    ]
    late = [
        pltpu.make_async_copy(src, dst, in_sem.at[4 + i])
        for i, (src, dst) in enumerate((
            (bias_h, bias), (norm_h, norm), (stab_h, stab), (past_k_h, past_k),
            (past_v_h, past_v), (past_i_h, past_i), (past_f_h, past_f), (taken_h, taken),
        ))
    ]
    big = [
        pltpu.make_async_copy(src, w_in.at[i], w_sem.at[min(i, 1)])
        for i, src in enumerate((w0_h, w1_h, w2_h, w3_h))
    ]
    load_out = pltpu.make_async_copy(wo_h, w_out, w_sem.at[2])

    def load(q):
        return pltpu.make_async_copy(memory_h.at[q], memory.at[q], m_sem)

    for copy in small + big + late:
        copy.start()
    load_out.start()
    each(seqs, lambda q: load(q).start())

    barrier = pltpu.get_barrier_semaphore()
    each(n, lambda i: signal(barrier, lax.rem(k + i, n), t), 1)
    each(m, lambda j: signal(barrier, k, lax.rem(t + j, m)), 1)
    def pair_core(y):
        return 2 * y + k % 2

    def is_me(kk, tt):
        return jnp.logical_and(kk == k, tt == t)

    def greet_root(h):
        @pl.when(jnp.logical_and(h != mine, jnp.logical_not(root)))
        def _():
            signal(barrier, t0 * r + h, t0)

    each(r, greet_root)

    @pl.when(jnp.logical_and(root_core, jnp.logical_not(root)))
    def _():
        def greet_source(j):
            @pl.when(j // r != t0)
            def _():
                signal(barrier, j, t0)

        each(n, greet_source)


    def greet_last(h):
        for y in range(pairs):
            @pl.when(jnp.logical_not(is_me(t * r + h, pair_core(y))))
            def _(y=y):
                signal(barrier, t * r + h, pair_core(y))

    each(r, greet_last)
    both = jnp.logical_and(root, k % 2 == core).astype(jnp.int32)
    pl.semaphore_wait(
        barrier,
        (n - 1) + (m - 1) + half - both
        + root.astype(jnp.int32) * ((r - 1) * (m - 1) - r * (pairs - 1))
        + r * (pairs - 1),
    )

    small[0].wait()

    def cousin(i):
        return lax.rem(t + 2 * i, m)

    def cut(h):
        return pl.ds(pl.multiple_of(h * width, width), width)

    def token_copy(h, i):
        return remote(
            tok.at[:, cut(h)], x_buf.at[k], t_send, x_recv.at[k], t * r + h, cousin(i)
        )

    def group_copy(h, tt):
        return remote(
            tok.at[:, cut(h)], x_buf.at[k], t_send, x_recv.at[k], t0 * r + h, tt
        )

    def group_each(act):
        def at_place(h):
            def to_tp(j):
                tt = lax.rem(t + j, m)

                @pl.when(jnp.logical_not(jnp.logical_and(h == mine, j == 0)))
                def _():
                    act(group_copy(h, tt))

            each(m, to_tp)

        each(r, at_place)

    @pl.when(root)
    def _():
        group_each(lambda copy: copy.start())
        x_buf[k] = tok[:, cut(mine)]

    @pl.when(jnp.logical_not(root))
    def _():
        for i in range(pairs):
            each(r, lambda h, i=i: token_copy(h, i).start())

    def forward(j):
        return remote(x_buf.at[j], x_buf.at[j], f_send, x_recv.at[j], k, partner)

    def pass_token(j):
        @pl.when(jnp.logical_not(jnp.logical_and(root, j == k)))
        def _():
            remote(
                tok.at[:, pl.ds(0, width)], x_buf.at[j], t_send, x_recv.at[j], k, t
            ).wait_recv()

        @pl.when(jnp.logical_and(root_core, j // r != t0))
        def _():
            forward(j).start()

    wg[pl.ds(2 * all_heads, wg.shape[0] - 2 * all_heads), :] = jnp.zeros(
        (wg.shape[0] - 2 * all_heads, local), bf16
    )
    for copy in small[1:]:
        copy.wait()
    floats = tok[...].astype(f32)
    squares = jnp.sum(floats * floats, axis=1, keepdims=True)
    lifted = floats * gain[:, pl.ds(pl.multiple_of(t * local, local), local)]
    raw = lax.dot_general(
        lifted.astype(bf16), wg[...], (((1,), (1,)), ((), ())), preferred_element_type=f32
    )
    lane = iota(raw.shape, 1)
    g_own[...] = jnp.where(lane < 2 * all_heads, raw, squares)

    def gate_copy(j):
        return remote(
            g_own, g_buf.at[j - 1], g_send, g_recv, k, lax.rem(t + j, m)
        )

    each(m, lambda j: gate_copy(j).start(), 1)
    own_gain = gain[:, pl.ds(pl.multiple_of(k * width, width), width)]

    def near_copy(c, i):
        return remote(give.at[c, i], near.at[c, i], n_send, n_recv.at[c, i], beside, t)

    def project(c, start, stop):
        both = xs[start:stop].reshape((stop - start) * 2 * rows, width)
        part = jnp.dot(both, w_in[c], preferred_element_type=f32).astype(bf16)
        for i in range(start, stop):
            at = (i - start) * 2 * rows
            give[c, i] = part[at : at + rows]
            keep[c, i] = part[at + rows : at + 2 * rows]

    def take_plane(p, i):
        for side, j in enumerate((p * 2 + 1 - x, p * 2 + x)):
            pass_token(j)
            xs[i, side * rows : (side + 1) * rows, :] = (
                x_buf[j].astype(f32) * own_gain
            ).astype(bf16)

    take_plane(z, 0)
    big[0].wait()
    project(0, 0, 1)
    near_copy(0, 0).start()
    pltpu.make_async_copy(w_in.at[pl.ds(1, 3)], w_in.at[pl.ds(1, 3)], w_sem.at[1]).wait()
    project(1, 0, 1)
    near_copy(1, 0).start()

    def far_plane(i):
        p = plane(i)
        take_plane(p, slot_of(p))

    each(half, far_plane, 1)
    project(0, 1, half)
    each(half, lambda i: near_copy(0, i).start(), 1)
    for c in range(1, 4):
        project(c, 1, half)

    def start_near(i):
        for c in range(1, 4):
            near_copy(c, i).start()

    each(half, start_near, 1)
    for c in range(2, 4):
        project(c, 0, 1)
        near_copy(c, 0).start()

    for copy in late:
        copy.wait()
    key_scale = dk ** (-0.5)
    reach = taken[...]
    chain_sum = jnp.zeros((heads, seqs), f32)
    running = []
    for j in range(chain):
        chain_sum = chain_sum + jnp.where(j < reach, log_sigmoid(past_f[j]), 0.0)
        running.append(chain_sum)
    carried_log = chain_sum + stab[...]
    new_stab = carried_log
    ends = []
    for j in range(chain):
        ends.append(jnp.where(j < reach, chain_sum - running[j] + past_i[j], -jnp.inf))
        new_stab = jnp.maximum(new_stab, ends[j])
    stab_new[...] = new_stab
    decay[...] = jnp.exp(carried_log - new_stab)
    for j in range(chain):
        weight_j = jnp.exp(ends[j] - new_stab)
        for h in range(heads):
            weights[h, j : j + 1, :] = weight_j[h : h + 1, :]

    remote(g_buf, g_buf, g_send, g_recv, k, t).wait_recv()
    total = g_own[...]
    for j in range(m - 1):
        total = total + g_buf[j]
    scale = lax.rsqrt(total[:, 2 * all_heads : 2 * all_heads + 1] / features + epsilon)
    gates = total * scale

    token_row = iota((rows, rows), 0)
    token_col = iota((rows, rows), 1)
    same_seq = token_row // chain == token_col // chain
    causal = jnp.logical_and(same_seq, token_col <= token_row)
    diagonal = token_row == token_col
    own_seq = iota((rows, seqs), 0) // chain == iota((rows, seqs), 1)
    first = t * heads

    def to_row(col):
        return jnp.sum(jnp.where(diagonal, col, 0.0), axis=0, keepdims=True)

    def pick(array, at):
        return jnp.sum(
            jnp.where(iota(array.shape, 1) == at, array, 0.0), axis=1, keepdims=True
        )

    for h in range(heads):
        in_col = pick(gates, first + h)
        forget = pick(gates, all_heads + first + h) + pick(bias[...], first + h)
        b_col = jnp.sum(
            jnp.where(causal, to_row(log_sigmoid(forget)), 0.0), axis=1, keepdims=True
        )
        within = jnp.where(causal, b_col + to_row(in_col - b_col), -jnp.inf)
        stab_col = jnp.sum(
            jnp.where(own_seq, stab_new[h : h + 1, :], 0.0), axis=1, keepdims=True
        )
        carried = b_col + stab_col
        stable = jnp.maximum(carried, jnp.max(within, axis=1, keepdims=True))
        spread[h] = jnp.exp(within - stable) * key_scale
        carries[h] = jnp.broadcast_to(jnp.exp(carried - stable), carries.shape[1:])

    def take(q):
        for h in range(heads):
            at = slice(h * dk, (h + 1) * dk)
            w_col = jnp.sum(
                jnp.where(iota((chain, seqs), 1) == q, weights[h], 0.0), axis=1, keepdims=True
            )
            fade = jnp.sum(
                jnp.where(iota((1, seqs), 1) == q, decay[h : h + 1, :], 0.0),
                axis=1, keepdims=True,
            )
            lifted_k = past_k[q, :, at].astype(f32) * key_scale * w_col
            norm_new[q, h : h + 1, :] = fade * norm[q, h : h + 1, :] + jnp.sum(
                lifted_k, axis=0, keepdims=True
            )
            added = lax.dot_general(
                lifted_k.astype(bf16),
                past_v[q, :, h * dv : (h + 1) * dv],
                (((0,), (0,)), ((), ())),
                preferred_element_type=f32,
            )
            new = fade * memory[q, h] + added
            memory[q, h] = new
            m_low[q, h] = new.astype(bf16)

    def line_copy(c, i):
        p = order(i)
        left = (p < z).astype(jnp.int32)
        slot = p + (p == z - 1).astype(jnp.int32) * (half - p)
        return remote(
            pair.at[c, i - 1], far.at[c, slot], z_send, z_recv.at[c, slot],
            (z + 1 - 2 * left) * 2 + x, t,
        )

    def line_wait(c, slot):
        remote(
            pair.at[c, 0], far.at[c, slot], z_send, z_recv.at[c, slot], k, t
        ).wait_recv()

    def fold(c, i):
        p = order(i)
        near_copy(c, i).wait_recv()
        starts = jnp.logical_or(
            jnp.logical_and(p > z, z == 0), jnp.logical_and(p < z, z == half - 1)
        )

        @pl.when(starts)
        def _():
            pair[c, i - 1] = (keep[c, i].astype(f32) + near[c, i].astype(f32)).astype(bf16)

        @pl.when(jnp.logical_not(starts))
        def _():
            line_wait(c, p)
            pair[c, i - 1] = (
                keep[c, i].astype(f32) + near[c, i].astype(f32) + far[c, p].astype(f32)
            ).astype(bf16)

        line_copy(c, i).start()

    pltpu.make_async_copy(memory_h, memory, m_sem).wait()

    def fold_query(i):
        fold(0, i)
        each(seqs * i // (half - 1), take, seqs * (i - 1) // (half - 1))

    each(half, fold_query, 1)

    def fold_rest(i):
        for c in range(1, 4):
            fold(c, i)

    each(half, fold_rest, 1)

    def settle(c, out):
        near_copy(c, 0).wait_recv()
        total_c[...] = keep[c, 0].astype(f32) + near[c, 0].astype(f32)

        def add(slot):
            line_wait(c, slot)
            total_c[...] += far[c, slot].astype(f32)

        @pl.when(z > 0)
        def _():
            add(z)

        @pl.when(z < half - 1)
        def _():
            add(half)

        out[...] = (total_c[...] * scale).astype(bf16)

    settle(0, query_b)
    row_seq = iota((rows, dv), 0) // chain
    from_memory[...] = jnp.zeros(from_memory.shape, f32)

    def recall(q):
        for h in range(heads):
            at = slice(h * dv, (h + 1) * dv)
            got = jnp.dot(
                query_b[:, h * dk : (h + 1) * dk], m_low[q, h], preferred_element_type=f32
            )
            from_memory[:, at] = jnp.where(row_seq == q, got, from_memory[:, at])

    each(seqs, recall)
    settle(1, key_b)

    scores, dens = [], []
    for h in range(heads):
        at = slice(h * dk, (h + 1) * dk)
        match = lax.dot_general(
            query_b[:, at], key_b[:, at], (((1,), (1,)), ((), ())), preferred_element_type=f32
        )
        score = match * spread[h]
        across_n = lax.dot_general(
            query_b[:, at].astype(f32), norm_new[:, h, :], (((1,), (1,)), ((), ())),
            precision=lax.Precision.HIGHEST, preferred_element_type=f32,
        )
        q_n = jnp.sum(jnp.where(own_seq, across_n, 0.0), axis=1, keepdims=True)
        den = carries[h, :, :1] * q_n + jnp.sum(score, axis=1, keepdims=True)
        scores.append(score.astype(bf16))
        dens.append(1.0 / jnp.maximum(jnp.abs(den), 1.0))

    settle(2, value_b)
    for h in range(heads):
        at = slice(h * dv, (h + 1) * dv)
        fresh = jnp.dot(scores[h], value_b[:, at], preferred_element_type=f32)
        from_memory[:, at] = (carries[h, :, :1] * from_memory[:, at] + fresh) * dens[h]
    settle(3, outgate_b)
    gated[...] = (jax.nn.sigmoid(outgate_b[...].astype(f32)) * from_memory[...]).astype(bf16)

    def along_copy(i):
        return remote(gated, a_buf.at[k], a_send, a_recv.at[k], plane(i) * 2 + x, t)

    def across_copy(i):
        at = plane(i) * 2 + x
        return remote(a_buf.at[at], a_buf.at[at], a_send, a_recv.at[at], beside, t)

    own_copy = remote(gated, a_buf.at[k], a_send, a_recv.at[k], beside, t)
    each(half, lambda i: along_copy(i).start(), 1)
    own_copy.start()
    a_buf[k] = gated[...]
    load_out.wait()

    def landed(at):
        remote(gated, a_buf.at[at], a_send, a_recv.at[at], k, t).wait_recv()

    def part_copy(p):
        return remote(
            p_buf.at[p * 2 + 1 - core], q_buf.at[p], p_send, p_recv.at[p], k, partner
        )

    def mix_plane(p):
        landed(p * 2 + 1 - x)
        both_rows = a_buf[pl.ds(p * 2, 2)].reshape(2 * rows, cols)
        part = jnp.dot(both_rows, w_out[...], preferred_element_type=f32).astype(bf16)
        for side in range(2):
            p_buf[p * 2 + side] = part[side * rows : (side + 1) * rows]
        part_copy(p).start()

    def final_copy(p):
        return remote(
            o_send.at[p], o_buf.at[mine, t // 2], o_ssem, o_rsem.at[mine, t // 2],
            p * 2 + core, t0,
        )

    def stays(p):
        return jnp.logical_and(root, p * 2 + core == k)

    def sum_plane(p):
        part_copy(p).wait_recv()
        o_send[p] = (
            p_buf[p * 2 + core].astype(f32) + q_buf[p].astype(f32)
        ).astype(bf16)

        @pl.when(jnp.logical_not(stays(p)))
        def _():
            final_copy(p).start()

        @pl.when(stays(p))
        def _():
            o_buf[mine, t // 2] = o_send[p]

    def pass_on(i):
        landed(plane(i) * 2 + x)
        across_copy(i).start()

    each(half - 1, pass_on, 1)
    mix_plane(z)
    if half > 1:
        pass_on(half - 1)

    def mix_next(i):
        mix_plane(plane(i))
        later = (i > 1).astype(jnp.int32)
        sum_plane(later * plane(i - 1) + (1 - later) * z)

    each(half - 1, mix_next, 1)
    mix_plane(plane(half - 1))
    if half > 1:
        sum_plane(plane(half - 2))
    sum_plane(plane(half - 1))
    for h in range(r):
        for y in range(pairs):
            @pl.when(jnp.logical_not(is_me(t * r + h, pair_core(y))))
            def _(h=h, y=y):
                remote(
                    o_send.at[0], o_buf.at[h, y], o_ssem, o_rsem.at[h, y], k, t
                ).wait_recv()

        summed = o_buf[h, 0].astype(f32)
        for y in range(1, pairs):
            summed = summed + o_buf[h, y].astype(f32)
        mixed[:, h * out_cols : (h + 1) * out_cols] = summed.astype(bf16)

    @pl.when(root)
    def _():
        sent = x_buf.at[pl.ds(0, n - 1)]
        remote(sent, sent, t_send, x_recv.at[0], k, t).wait_send()

    @pl.when(jnp.logical_not(root))
    def _():
        sent = x_buf.at[pl.ds(0, r * pairs)]
        remote(sent, sent, t_send, x_recv.at[0], k, t).wait_send()

    @pl.when(root_core)
    def _():
        sent = x_buf.at[pl.ds(0, n - r)]
        remote(sent, sent, f_send, x_recv.at[0], k, t).wait_send()

    remote(g_buf, g_buf, g_send, g_recv, k, t).wait_send()
    remote(give, give, n_send, n_recv.at[0, 0], k, t).wait_send()
    remote(pair, pair, z_send, z_recv.at[0, 0], k, t).wait_send()
    sent = a_buf.at[pl.ds(0, n - 1)]
    remote(sent, sent, a_send, a_recv.at[0], k, t).wait_send()
    remote(q_buf, q_buf, p_send, p_recv.at[0], k, t).wait_send()
    keeps = jnp.logical_and(root, k % 2 == core)

    @pl.when(keeps)
    def _():
        sent = o_send.at[pl.ds(0, half - 1)]
        remote(sent, sent, o_ssem, o_rsem.at[0, 0], k, t).wait_send()

    @pl.when(jnp.logical_not(keeps))
    def _():
        remote(o_send, o_send, o_ssem, o_rsem.at[0, 0], k, t).wait_send()


def cell(n, m, tokens, gain, wi, wf, bias, weights, w_out, memory, norm, stab, past_k, past_v,
         past_i, past_f, taken):
    seqs, heads, dk, dv = memory.shape
    rows, local = tokens.shape
    width, cols = weights[0].shape
    all_heads = wi.shape[0]
    chain = past_k.shape[1]
    depth, out_cols = w_out.shape
    half, r = n // 2, n // m
    lanes = -(-(2 * all_heads + 1) // 128) * 128
    V = pltpu.VMEM
    outs = [
        V((rows, local), bf16), V((rows, cols), bf16), V((rows, cols), bf16),
        V(memory.shape, f32), V(norm.shape, f32), V(stab.shape, f32),
    ]
    return pl.pallas_call(
        functools.partial(cell_kernel, n, m, all_heads, local * m, chain),
        out_shape=outs,
        in_specs=[hbm] * 18,
        out_specs=[vmem] * 6,
        scratch_shapes=[
            V((rows, local), bf16), V(gain.shape, f32), V((lanes, local), bf16),
            V(bias.shape, f32), V((4, width, cols), bf16), V(w_out.shape, bf16),
            V(norm.shape, f32), V(stab.shape, f32), V(past_k.shape, bf16),
            V(past_v.shape, bf16), V(past_i.shape, f32), V(past_f.shape, f32),
            V(taken.shape, jnp.int32),
            V((n, rows, width), bf16), V((half, 2 * rows, width), bf16),
            V((4, half, rows, cols), bf16), V((4, half, rows, cols), bf16),
            V((4, half, rows, cols), bf16), V((4, half - 1, rows, cols), bf16),
            V((4, half + 1, rows, cols), bf16), V((rows, cols), f32),
            V((rows, lanes), f32), V((m - 1, rows, lanes), f32),
            V(memory.shape, bf16), V((heads, chain, seqs), f32), V(stab.shape, f32),
            V((heads, rows, rows), f32), V((heads, rows, 128), f32),
            V((rows, cols), bf16), V((rows, cols), bf16), V((rows, cols), f32),
            V((rows, cols), bf16),
            V((n, rows, cols), bf16), V((n, rows, out_cols), bf16),
            V((half, rows, out_cols), bf16), V((half, rows, out_cols), bf16),
            V((r, m // 2, rows, out_cols), bf16),
            DMA((12,)), DMA((3,)), DMA, DMA, DMA, DMA((n,)), DMA, DMA,
            DMA, DMA((4, half)), DMA, DMA((4, half + 1)),
            DMA, DMA((n,)), DMA, DMA((half,)), DMA, DMA((r, m // 2)),
        ],
        compiler_params=pltpu.CompilerParams(
            collective_id=0, has_side_effects=True, vmem_limit_bytes=40 * 1024 * 1024
        ),
    )(*(pltpu.with_memory_space_constraint(a, pltpu.HBM) for a in (
        tokens, gain, wi, wf, bias, *weights, w_out, memory, norm, stab, past_k, past_v,
        past_i, past_f, taken,
    )))


def put_kernel(count, pieces, *refs):
    sems = refs[-1]
    copies = []
    at = 0
    for src, dst, cut in zip(refs[:count], refs[count : 2 * count], pieces):
        for piece in range(cut):
            a, b = (src.at[piece], dst.at[piece]) if cut > 1 else (src, dst)
            copies.append(pltpu.make_async_copy(a, b, sems.at[at]))
            at += 1
    for copy in copies:
        copy.start()
    for copy in copies:
        copy.wait()


def put(arrays, pieces):
    return pl.pallas_call(
        functools.partial(put_kernel, len(arrays), pieces),
        out_shape=[jax.ShapeDtypeStruct(a.shape, a.dtype) for a in arrays],
        in_specs=[vmem] * len(arrays),
        out_specs=[hbm] * len(arrays),
        scratch_shapes=[DMA((sum(pieces),))],
        compiler_params=pltpu.CompilerParams(vmem_limit_bytes=16 * 1024 * 1024),
    )(*arrays)


def body(
    n, m, tokens, norm_gain, query_weight, key_weight, value_weight, outgate_weight,
    ingate_weight, forget_weight, forget_bias, output_weight, state_memory, state_normaliser,
    state_stabiliser, past_keys, past_values, past_ingate, past_forget, accepted,
):
    outs = cell(
        n, m, tokens, norm_gain[None, :], ingate_weight.T, forget_weight.T,
        forget_bias[None, :], (query_weight, key_weight, value_weight, outgate_weight),
        output_weight, state_memory, state_normaliser, state_stabiliser.T, past_keys,
        past_values, past_ingate.transpose(1, 2, 0), past_forget.transpose(1, 2, 0),
        accepted[None, :],
    )
    mixed, keys, values, memory, normaliser, stabiliser = put(
        outs, (1, 1, 1, state_memory.shape[0], 1, 1)
    )
    return (mixed, memory, normaliser, stabiliser.T, keys, values)


def solution(mesh):
    rows = P("kv", "tp")
    chained = P("kv", None, "tp")
    return jax.shard_map(
        functools.partial(body, mesh.shape["kv"], mesh.shape["tp"]),
        mesh=mesh,
        in_specs=(
            rows, P(), rows, rows, rows, rows, P(), P(), P(), P("tp", "kv"),
            P("kv", "tp", None, None), P("kv", "tp", None), rows,
            chained, chained, chained, chained, P("kv"),
        ),
        out_specs=(
            rows, P("kv", "tp", None, None), P("kv", "tp", None), rows, rows, rows,
        ),
        check_vma=False,
    )
```
